32 devices in a mesh: grp: 2 (over y), ep: 8 (over z, x), tp: 2 (over core).
Axes of the slice: x: 2, y: 2, z: 4, core: 2. Of those that a mesh axis runs over, the one named last changes fastest.
Arguments:
- tokens: bfloat16 [8192, 2048], P(('grp', 'ep', 'tp')), parts along dimension 0, may hold values from -15 to 15
- gain_in: float32 [2048], replicated, may hold values from 0.1 to 1.9
- expert_ids: int32 [8192, 2], P(('grp', 'ep')), parts along dimension 0, may hold values from 0 to 7, all different within a row; in each aligned block of 256 rows (0 to 255, 256 to 511, ...) at most 128 rows name the same one
- gate_weights: float32 [8192, 2], P(('grp', 'ep')), parts along dimension 0, may hold values from 0.1 to 1
- w_gate: bfloat16 [8, 2048, 512], P('ep', None, 'tp'), may hold values from -0.125 to 0.125
- w_up: bfloat16 [8, 2048, 512], P('ep', None, 'tp'), may hold values from -0.125 to 0.125
- w_down: bfloat16 [8, 2048, 512], P('ep', None, 'tp'), may hold values from -20 to 20
- gain_out: float32 [2048], P('tp'), may hold values from 0.1 to 1.9
Outputs:
- mixed: bfloat16 [8192, 2048], P(('grp', 'ep'), 'tp'), parts along dimension 0
The draws below stay inside these ranges and needn't reach their ends.
There are 2 independent parts, one for each index of `grp`. The reference program is written for one: setup_inputs(seed, part) draws one part's arguments, and reference() takes and returns one part's arrays. A program takes and returns all parts, laid end to end along the dimension named above; an argument that names none is the same for every part. Nothing has to cross between parts.
Inputs may be any that keep to these rules, and one draw needn't show every extreme that they name: `expert_ids`: each token names 2 different experts; in each aligned block of 256 tokens no expert is named by more than 128 pairs, a bound that some block reaches.
All inputs are finite; a program needn't handle non-finite values.
Results may differ from the reference program's by a relative error of at most 0.0077.
Values may be sent and summed in bfloat16 or wider, within the bound.
A program may use at most 64 MiB of HBM per device.

```python
import math
import jax
import jax.numpy as jnp
import numpy as np
from jax import lax

D = 2048
DE = 512
TOP_K = 2
TOK_DEV = 256
EXPERTS = 8
CAP = 128
HALVES = 2
TOKENS = 4096


def draw_w_down(key, part):
    jitter = jax.random.uniform(jax.random.fold_in(key, 12), (D,), jnp.float32, 0.6, 1.4)
    column = jnp.arange(D, dtype=jnp.float32) / D
    base = jnp.clip(jax.random.normal(jax.random.fold_in(key, 11), (EXPERTS, D, DE), jnp.float32), -4.0, 4.0)
    rise = 10.0 ** column
    values = base * (rise * jitter)[None, :, None] * DE ** (-0.5)
    return jnp.clip(values, -20.0, 20.0).astype(jnp.bfloat16)


def block_levels(rng, shape, pieces, smallest, top_value):
    gain = 1.0
    for dim, blocks in pieces:
        steps = jax.random.uniform(jax.random.fold_in(jax.random.fold_in(rng, 6), dim), (blocks,), jnp.float32, smallest / len(pieces), top_value / len(pieces))
        gain = gain * jnp.repeat(jnp.exp(steps), shape[dim] // blocks).reshape((-1,) + (1,) * (len(shape) - 1 - dim))
    return gain


def assign_block(stream_key, own, number, rows, number_of, top, reach, slope):
    sequence = jax.random.permutation(stream_key, number_of)
    heavy_load, ordinary = shares(number_of, rows * top, reach, slope, True), shares(number_of, rows * top, reach, slope, False)
    places = jnp.arange(number_of)

    def named(sizes, offset_by):
        used = int((sizes > 0).sum())
        fixed = max(1, used // 4)
        moved = fixed + (places - fixed + offset_by * (used - fixed)) % max(1, number_of - fixed)
        return jnp.zeros((number_of,), jnp.int32).at[sequence[jnp.where(places < fixed, places, moved)]].set(jnp.asarray(sizes, jnp.int32))

    sizes = jnp.where(number % 4 == 0, named(heavy_load, number // 4), named(ordinary, number - number // 4 - 1))
    mixed = jax.random.permutation(jax.random.fold_in(own, 3), number_of)
    source_of, receiver = mixed[0:number_of // 2 * 2:2], mixed[1:number_of // 2 * 2:2]
    room = jnp.minimum(sizes[source_of] - 1, reach - sizes[receiver]) // 2
    room = jnp.where((source_of == sequence[0]) | (receiver == sequence[0]) | (sizes[receiver] == 0), 0, jnp.maximum(room, 0))
    moved = jax.random.randint(jax.random.fold_in(own, 4), (number_of // 2,), 0, 1 << 20) % (room + 1)
    sizes = sizes.at[source_of].add(-moved).at[receiver].add(moved)
    items = jnp.searchsorted(jnp.cumsum(sizes), jnp.arange(rows * top), side="right").astype(jnp.int32)
    table = items.reshape(top, rows).T
    table = table[jax.random.permutation(jax.random.fold_in(own, 1), rows)]
    offset_by = jax.random.randint(jax.random.fold_in(own, 2), (rows, 1), 0, top)
    return jnp.take_along_axis(table, (jnp.arange(top)[None, :] + offset_by) % top, axis=1)


def shares(amount, total, most, lean, full):
    portions = [(1 << 20) // math.isqrt(grade ** lean) + 1 for grade in range(1, amount + 1)]
    largest = most if full else min(most, max(-(-total // amount), total * portions[0] // sum(portions)))
    least = 1 if total - largest >= amount - 1 else 0
    given, spare = [largest] + [least] * (amount - 1), total - largest - least * (amount - 1)
    while spare > 0:
        movable = [i for i in range(1, amount) if given[i] < largest] or [i for i in range(1, amount) if given[i] < most]
        whole, left = sum([portions[i] for i in movable]), spare
        for i in movable:
            addition = min(most - given[i], max(1, left * portions[i] // whole), spare)
            given[i] = given[i] + addition
            spare = spare - addition
    return np.array(given)


def gaussian(rng, dims, spread, most, shards=(), kind=jnp.bfloat16):
    result = jax.random.normal(rng, dims, jnp.float32) * spread
    if len(shards) > 0:
        result = block_levels(rng, dims, shards, -0.22, 0.18) * result
    return jnp.clip(result, min=-most, max=most).astype(kind)


def setup_inputs(seed: int = 0, part: int = 0) -> dict:
    seeds = jax.random.split(jax.random.key(seed), 9)
    part_splits = jax.random.split(jax.random.fold_in(seeds[8], part), 9)
    tokens = gaussian(part_splits[0], (TOKENS, D), 3.0, 15.0, ((0, 16),))
    gain_in = jnp.clip(1.0 + 0.18 * jax.random.normal(seeds[1], (D,), jnp.float32), 0.1, 1.9)
    expert_ids_keys = jax.random.split(jax.random.fold_in(part_splits[2], 1), TOKENS // TOK_DEV)
    expert_ids_turns = jax.random.permutation(jax.random.fold_in(part_splits[2], 3), TOKENS // TOK_DEV)
    expert_ids = jax.vmap(lambda own, number: assign_block(jax.random.fold_in(part_splits[2], 2), own, number, TOK_DEV, EXPERTS, TOP_K, CAP, 2))(expert_ids_keys, expert_ids_turns).reshape((TOKENS, TOP_K))
    gate_weights = jnp.clip(jnp.exp(math.log(1.0) - 2.3025851 * jax.random.uniform(part_splits[3], (TOKENS, TOP_K), jnp.float32) ** block_levels(part_splits[3], (TOKENS, TOP_K), ((0, 8),), -0.2, 0.2)), 0.1, 1.0)
    w_gate = gaussian(seeds[4], (EXPERTS, D, DE), D ** -0.5, 0.125, ((0, 8), (2, 2)))
    w_up = gaussian(seeds[5], (EXPERTS, D, DE), D ** -0.5, 0.125, ((0, 8), (2, 2)))
    w_down = draw_w_down(jax.random.fold_in(seeds[8], 71), part)
    gain_out = jnp.clip(1.0 + 0.18 * jax.random.normal(seeds[7], (D,), jnp.float32), 0.1, 1.9)
    return dict(tokens=tokens, gain_in=gain_in, expert_ids=expert_ids, gate_weights=gate_weights, w_gate=w_gate, w_up=w_up, w_down=w_down, gain_out=gain_out)


EPS = 1e-06

def block_slots(expert_ids, block_rows, experts):
    pairs = expert_ids.reshape(-1, block_rows * expert_ids.shape[1])
    onehot = (pairs[:, :, None] == jnp.arange(experts, dtype=jnp.int32)[None, None, :]).astype(jnp.int32)
    before = jnp.cumsum(onehot, axis=1) - onehot
    return lax.optimization_barrier(jnp.sum(before * onehot, axis=2)).reshape(expert_ids.shape).astype(jnp.int32)

def reference(tokens, gain_in, expert_ids, gate_weights, w_gate, w_up, w_down, gain_out):
    x_float = tokens.astype(jnp.float32)
    normed = (x_float * lax.rsqrt(lax.optimization_barrier(jnp.mean(x_float * x_float, axis=1, keepdims=True)) + EPS) * gain_in).astype(jnp.bfloat16)
    slots = block_slots(expert_ids, TOK_DEV, EXPERTS)
    sources = TOKENS // TOK_DEV
    token_ids = jnp.broadcast_to(jnp.arange(TOKENS, dtype=jnp.int32)[:, None], expert_ids.shape)
    position = token_ids // TOK_DEV * CAP + slots
    table = jnp.full((EXPERTS, sources * CAP), TOKENS, jnp.int32).at[expert_ids, position].set(token_ids)
    row_gates = jnp.zeros((EXPERTS, sources * CAP), jnp.float32).at[expert_ids, position].set(gate_weights)
    padded = jnp.concatenate([normed, jnp.zeros((1, D), jnp.bfloat16)], axis=0)
    block = DE // HALVES

    def one_expert(total, inputs):
        rows_index, gates_here, gate_matrix, up_matrix, down_matrix = inputs
        rows = padded[rows_index]
        gated = jnp.dot(rows, gate_matrix, preferred_element_type=jnp.float32)
        upward = jnp.dot(rows, up_matrix, preferred_element_type=jnp.float32)
        hidden = (jax.nn.silu(gated) * upward).astype(jnp.bfloat16)
        summed = jnp.zeros((rows.shape[0], D), jnp.float32)
        for index in range(HALVES):
            part = lax.dot_general(hidden[:, index * block:(index + 1) * block], down_matrix[:, index * block:(index + 1) * block], (((1,), (1,)), ((), ())), preferred_element_type=jnp.float32)
            summed = summed + lax.optimization_barrier(part.astype(jnp.bfloat16)).astype(jnp.float32)
        expert_out = summed.astype(jnp.bfloat16).astype(jnp.float32)
        return (total.at[rows_index].add(gates_here[:, None] * expert_out), None)
    combined, _ = lax.scan(one_expert, jnp.zeros((TOKENS + 1, D), jnp.float32), (table, row_gates, w_gate, w_up, w_down))
    combined = combined[:TOKENS]
    inverse = lax.rsqrt(lax.optimization_barrier(jnp.mean(combined * combined, axis=1, keepdims=True)) + EPS)
    return (combined * inverse * gain_out).astype(jnp.bfloat16)
```

```python
import functools

import jax
import jax.numpy as jnp
from jax import lax
from jax.experimental import pallas as pl
from jax.experimental.pallas import tpu as pltpu
from jax.sharding import PartitionSpec as P

EPS = 1e-06
MESH = pl.DeviceIdType.MESH
NT = (((1,), (1,)), ((), ()))
TN = (((0,), (0,)), ((), ()))


def plane_width(ep):
    return max(n for n in range(1, ep + 1) if ep % n == 0 and n**3 <= ep)


def kernel(
    G, X, Z, F, cap,
    tokens_ref, gain_in_ref, meta_ref, wg_ref, wu_ref, wd_ref, gain_out_ref,
    out_ref,
    wbuf, tok, meta, acc, comb, rows, hid, pick, gslot, gains, inbox,
    wsem, wx_send, wy_send, wt_send, tok_recv, tok_send, meta_recv, meta_send,
    acc_recv, acc_send, misc_recv, misc_send, load_sem,
):
    g, ep, c = lax.axis_index("grp"), lax.axis_index("ep"), lax.axis_index("tp")
    z, x = ep // X, lax.rem(ep, X)
    other = 1 - c
    T = tokens_ref.shape[0]
    D = tokens_ref.shape[1]
    C = D // F
    H = wg_ref.shape[-1]
    FG = F // G
    weights = (wg_ref, wu_ref, wd_ref)

    def arrived(ref, sem):
        pltpu.make_async_copy(ref, ref, sem).wait()

    def send(src, dst, ssem, rsem, **where):
        return pltpu.make_async_remote_copy(
            src_ref=src, dst_ref=dst, send_sem=ssem, recv_sem=rsem,
            device_id=where, device_id_type=MESH,
        )

    def wslice(p, half, kind, q):
        return wbuf.at[p, half, kind, q]

    def load(f):
        return pltpu.make_async_copy(tokens_ref.at[:, f * C : (f + 1) * C], tok.at[z, f], load_sem.at[f])

    for f in range(F):
        load(f).start()

    for kind in range(3):
        for q in range(F):
            pltpu.make_async_copy(
                weights[kind].at[q], wslice(x, c, kind, q), wsem.at[x, c, kind, q]
            ).start()

    barrier = pltpu.get_barrier_semaphore()
    for i in range(1, Z):
        pl.semaphore_signal(barrier, inc=1, device_id={"ep": lax.rem(z + i, Z) * X + x}, device_id_type=MESH)
    for i in range(1, X):
        pl.semaphore_signal(barrier, inc=1, device_id={"ep": z * X + lax.rem(x + i, X)}, device_id_type=MESH)
    for i in range(1, G):
        pl.semaphore_signal(barrier, inc=1, device_id={"grp": lax.rem(g + i, G)}, device_id_type=MESH)
    pl.semaphore_signal(barrier, inc=1, device_id={"tp": other}, device_id_type=MESH)

    square = jnp.zeros((T, 1), jnp.float32)
    for f in range(F):
        load(f).wait()
        value = tok[z, f].astype(jnp.float32)
        square = square + jnp.sum(value * value, axis=1, keepdims=True)
    inv = lax.rsqrt(square / D + EPS)
    for f in range(F):
        gain = gain_in_ref[:, f * C : (f + 1) * C]
        tok[z, f] = (tok[z, f].astype(jnp.float32) * inv * gain).astype(jnp.bfloat16)

    pl.semaphore_wait(barrier, Z + X + G - 2)

    def to_line(i):
        return send(
            meta_ref, meta.at[z], meta_send.at[i], meta_recv.at[z], ep=lax.rem(z + i, Z) * X + x
        )

    for i in range(1, Z):
        to_line(i).start()

    def along(b, f, way):
        step = 1 if way == 0 else -1
        return send(
            tok.at[b, f], tok.at[b, f], tok_send.at[way, b, f], tok_recv.at[b, f], ep=(z + step) * X + x
        )

    can = (z < Z - 1, z > 0)
    for f in range(F):
        for way in range(2):
            pl.when(can[way])(lambda f=f, way=way: along(z, f, way).start())

    def to_plane(i, kind, j):
        q = g * FG + j
        return send(
            weights[kind].at[q], wslice(x, c, kind, q), wx_send.at[i, kind, j],
            wsem.at[x, c, kind, q], ep=z * X + lax.rem(x + i, X),
        )

    for kind in range(3):
        for j in range(FG):
            for i in range(1, X):
                to_plane(i, kind, j).start()

    gain_copy = send(gain_out_ref, gains.at[1], misc_send.at[0], misc_recv.at[0], tp=other)
    gain_copy.start()
    gains[0] = gain_out_ref[...]
    meta[z] = meta_ref[...]

    def to_core(p, kind, q):
        return send(
            wslice(p, c, kind, q), wslice(p, c, kind, q), wt_send.at[p, kind, q],
            wsem.at[p, c, kind, q], tp=other,
        )

    def to_group(p, i, kind, j):
        q = g * FG + j
        return send(
            wslice(p, c, kind, q), wslice(p, c, kind, q), wy_send.at[p, i, kind, j],
            wsem.at[p, c, kind, q], grp=lax.rem(g + i, G),
        )

    for kind in range(3):
        for q in range(F):
            arrived(wslice(x, c, kind, q), wsem.at[x, c, kind, q])
            to_core(x, kind, q).start()

    def from_plane(n):
        kind, j = n // FG, n % FG
        q = g * FG + j
        for i in range(1, X):
            p = lax.rem(x + i, X)
            arrived(wslice(p, c, kind, q), wsem.at[p, c, kind, q])
            for i2 in range(1, G):
                to_group(p, i2, kind, j).start()
            to_core(p, kind, q).start()

    def from_group(n):
        kind, j = n // FG, n % FG
        for i in range(1, X):
            p = lax.rem(x + i, X)
            for i2 in range(1, G):
                q = lax.rem(g + i2, G) * FG + j
                arrived(wslice(p, c, kind, q), wsem.at[p, c, kind, q])
                to_core(p, kind, q).start()

    def from_core(kind):
        for p in range(X):
            for q in range(F):
                arrived(wslice(p, other, kind, q), wsem.at[p, other, kind, q])

    def relay(d, f):
        for way in range(2):
            b = z - d if way == 0 else z + d
            have = b >= 0 if way == 0 else b < Z

            @pl.when(have)
            def _():
                arrived(tok.at[b, f], tok_recv.at[b, f])
                pl.when(can[way])(lambda: along(b, f, way).start())

    def hidden(b):
        m = meta[b]
        expert = (lax.broadcasted_iota(jnp.int32, (8, T), 0) + z * X).astype(jnp.float32)
        first, second = m[0:1] == expert, m[1:2] == expert
        named = jnp.where(first | second, 1.0, 0.0)
        gate = jnp.where(first, m[2:3], 0.0) + jnp.where(second, m[3:4], 0.0)
        line = lax.broadcasted_iota(jnp.int32, (T, T), 0)
        earlier = jnp.where(line < lax.broadcasted_iota(jnp.int32, (T, T), 1), 1.0, 0.0)
        before = jnp.dot(
            named.astype(jnp.bfloat16), earlier.astype(jnp.bfloat16), preferred_element_type=jnp.float32
        )
        place = jnp.where(named > 0.0, before, -1.0)
        slot = lax.broadcasted_iota(jnp.int32, (cap, T), 0).astype(jnp.float32)
        for p in range(X):
            hit = place[p : p + 1] == slot
            pick[b, p * cap : (p + 1) * cap] = jnp.where(hit, 1.0, 0.0).astype(jnp.bfloat16)
            weight = jnp.sum(jnp.where(hit, gate[p : p + 1], 0.0), axis=1, keepdims=True)
            gslot[b, p * cap : (p + 1) * cap] = jnp.broadcast_to(weight, (cap, 128))
        for f in range(F):
            rows[:, f * C : (f + 1) * C] = jnp.dot(
                pick[b], tok[b, f], preferred_element_type=jnp.float32
            ).astype(jnp.bfloat16)
        for p in range(X):
            here = rows[p * cap : (p + 1) * cap]
            for half in range(2):
                gated = jnp.dot(here, wbuf[p, half, 0].reshape(D, H), preferred_element_type=jnp.float32)
                up = jnp.dot(here, wbuf[p, half, 1].reshape(D, H), preferred_element_type=jnp.float32)
                value = gated / (1.0 + jnp.exp(-gated)) * up
                hid[b, p * cap : (p + 1) * cap, half * H : (half + 1) * H] = value.astype(jnp.bfloat16)

    def partial(b, f):
        parts = []
        for p in range(X):
            span = slice(p * cap, (p + 1) * cap)
            y = lax.dot_general(
                hid[b, span, 0:H], wbuf[p, 0, 2, f], NT, preferred_element_type=jnp.float32
            ) + lax.dot_general(
                hid[b, span, H : 2 * H], wbuf[p, 1, 2, f], NT, preferred_element_type=jnp.float32
            )
            parts.append((y * gslot[b, span, 0:1]).astype(jnp.bfloat16))
        return lax.dot_general(
            pick[b], jnp.concatenate(parts, axis=0), TN, preferred_element_type=jnp.float32
        )

    def both_hidden(d):
        def side(s, carry):
            b = z + d * (2 * s - 1)
            pl.when((b >= 0) & (b < Z))(lambda: hidden(b))
            return carry

        lax.fori_loop(0, 2, side, 0)

    def onward(b, f, way):
        step = 1 - 2 * way
        to = jnp.where((way == 1) & (z - 1 == b), Z, b)
        return send(
            acc.at[b, f], acc.at[to, f], acc_send.at[b, f], acc_recv.at[to, f], ep=(z + step) * X + x
        )

    def sums(d, low, high):
        def chunk(i, carry):
            f = i // 2
            turn = lax.rem(i, 2)
            way = jnp.where(2 * z < Z, turn, 1 - turn)
            b = jnp.where(way == 0, d, Z - 1 - d)
            active = jnp.where(way == 0, b - z, z - b) > 0
            fed = jnp.where(way == 0, z, Z - 1 - z) > 0

            @pl.when(active & fed)
            def _():
                part = partial(b, f)
                arrived(acc.at[b, f], acc_recv.at[b, f])
                acc[b, f] = (part + acc[b, f].astype(jnp.float32)).astype(jnp.bfloat16)
                onward(b, f, way).start()

            @pl.when(active & jnp.logical_not(fed))
            def _():
                acc[b, f] = partial(b, f).astype(jnp.bfloat16)
                onward(b, f, way).start()

            return carry

        lax.fori_loop(2 * low, 2 * high, chunk, 0)

    pieces = 3 * FG
    for n in range(max(pieces, F)):
        if n < F:
            relay(1, n)
        elif Z > 2 and n - F < F:
            relay(2, n - F)
        if n < pieces:
            from_plane(n)
        if 1 <= n <= pieces:
            from_group(n - 1)
    if pieces >= F:
        from_group(pieces - 1)
    done = max(pieces, F) - F
    for i in range(1, Z):
        b = lax.rem(z + i, Z)
        arrived(meta.at[b], meta_recv.at[b])
    from_core(0)
    from_core(1)
    both_hidden(1)
    from_core(2)
    early = F // 4
    sums(1, 0, early)
    if Z > 2:
        for f in range(done, F):
            relay(2, f)
        both_hidden(2)

    if Z > 2:
        sums(2, 0, F)

    def stage(d, carry):
        def one(f, inner):
            relay(d, f)
            return inner

        lax.fori_loop(0, F, one, 0)
        both_hidden(d)
        sums(d, 0, F)
        return carry

    lax.fori_loop(3, Z, stage, 0)
    sums(1, early, F)

    hidden(z)
    total = jnp.zeros((T, 1), jnp.float32)
    for f in range(F):
        comb[f] = partial(z, f)
    for f in range(F):

        @pl.when(z > 0)
        def _():
            arrived(acc.at[z, f], acc_recv.at[z, f])
            comb[f] = comb[f] + acc[z, f].astype(jnp.float32)

        @pl.when(z < Z - 1)
        def _():
            arrived(acc.at[Z, f], acc_recv.at[Z, f])
            comb[f] = comb[f] + acc[Z, f].astype(jnp.float32)

        value = comb[f]
        total = total + jnp.sum(value * value, axis=1, keepdims=True)
    scale = lax.rsqrt(total / D + EPS)
    arrived(gains.at[1], misc_recv.at[0])
    half = F // 2
    for f in range(F):
        pl.when(can[0])(lambda f=f: along(z, f, 0).wait_send())
        pl.when(can[1])(lambda f=f: along(z, f, 1).wait_send())
    for f in range(half):
        gain = gains[1, :, f * C : (f + 1) * C]
        tok[z, f] = (comb[other * half + f] * scale * gain).astype(jnp.bfloat16)
    out_copy = send(tok.at[z, :half], inbox, misc_send.at[1], misc_recv.at[1], tp=other)
    out_copy.start()
    for f in range(half):
        gain = gains[0, :, f * C : (f + 1) * C]
        out_ref[c, :, f * C : (f + 1) * C] = (comb[c * half + f] * scale * gain).astype(jnp.bfloat16)

    gain_copy.wait_send()
    for i in range(1, Z):
        to_line(i).wait_send()
    for kind in range(3):
        for i in range(1, X):
            p = lax.rem(x + i, X)
            for j in range(FG):
                to_plane(i, kind, j).wait_send()
                for i2 in range(1, G):
                    to_group(p, i2, kind, j).wait_send()
        for p in range(X):
            for q in range(F):
                to_core(p, kind, q).wait_send()

    def drain(b, carry):
        for f in range(F):
            pl.when(can[0] & (b < z))(lambda f=f: along(b, f, 0).wait_send())
            pl.when(can[1] & (b > z))(lambda f=f: along(b, f, 1).wait_send())
            pl.when(b != z)(lambda f=f: onward(b, f, 0).wait_send())
        return carry

    lax.fori_loop(0, Z, drain, 0)
    out_copy.wait()
    for f in range(half):
        out_ref[other, :, f * C : (f + 1) * C] = inbox[f]


def quad_kernel(
    G, X, Z, F, cap,
    tokens_ref, gain_in_ref, ids_ref, gates_ref, wg_ref, wu_ref, wd_ref, gain_out_ref,
    out_ref,
    wbuf, tok, meta, acc, comb, rows, gated, hid, pick, gslot, gains, stage, ids, gates,
    own_sem, nat_sem, plane_sem, group_sem, wide_sem, down_sem, wx_send, wy_send, wt_send,
    tok_recv, tok_send, meta_recv, meta_send, acc_recv, acc_send,
    gain_recv, gain_send, out_recv, out_send, load_sem, pair_sem,
):
    g, ep, c = lax.axis_index("grp"), lax.axis_index("ep"), lax.axis_index("tp")
    z, x = ep // X, lax.rem(ep, X)
    other = 1 - c
    T, D = tokens_ref.shape
    C = D // F
    W, C2, H = wg_ref.shape
    R = X * cap
    FG, WG = F // G, W // G
    SUB = W // F
    LEAD = F // 2
    LAG = 3
    weights = (wg_ref, wu_ref, wd_ref)
    is_end = (z == 0) | (z == Z - 1)
    is_inner = jnp.logical_not(is_end)
    s = jnp.where(2 * z < Z, 1, -1)
    IN, OUT = 0, 1

    def arrived(ref, sem):
        pltpu.make_async_copy(ref, ref, sem).wait()

    def send(src, dst, ssem, rsem, **where):
        return pltpu.make_async_remote_copy(
            src_ref=src, dst_ref=dst, send_sem=ssem, recv_sem=rsem,
            device_id=where, device_id_type=MESH,
        )

    def load(f):
        return pltpu.make_async_copy(tokens_ref.at[:, f * C : (f + 1) * C], tok.at[z, f], load_sem)

    def load_own(kind):
        return pltpu.make_async_copy(weights[kind], wbuf.at[x, c, kind], own_sem.at[kind])

    mine = pl.ds(pl.multiple_of(c * T, T), T)
    load_ids = pltpu.make_async_copy(ids_ref.at[:, mine], ids, pair_sem.at[0])
    load_gates = pltpu.make_async_copy(gates_ref.at[:, mine], gates, pair_sem.at[1])
    load_ids.start()
    load_gates.start()
    for f in range(F):
        load(f).start()
    for kind in range(3):
        load_own(kind).start()

    barrier = pltpu.get_barrier_semaphore()
    for i in range(1, Z):
        pl.semaphore_signal(barrier, inc=1, device_id={"ep": lax.rem(z + i, Z) * X + x}, device_id_type=MESH)
    for i in range(1, X):
        pl.semaphore_signal(barrier, inc=1, device_id={"ep": z * X + lax.rem(x + i, X)}, device_id_type=MESH)
    for i in range(1, G):
        pl.semaphore_signal(barrier, inc=1, device_id={"grp": lax.rem(g + i, G)}, device_id_type=MESH)
    pl.semaphore_signal(barrier, inc=1, device_id={"tp": other}, device_id_type=MESH)
    load_ids.wait()
    load_gates.wait()
    meta[z] = jnp.concatenate(
        [ids[...].astype(jnp.float32), gates[...], jnp.zeros((4, T), jnp.float32)], axis=0
    )
    gains[0] = gain_out_ref[...]
    arrived(tok.at[z], load_sem)
    load_own(0).wait()
    pl.semaphore_wait(barrier, Z + X + G - 2)

    def along(b, f, way):
        step = s if way == IN else -s
        return send(
            tok.at[b, f], tok.at[b, f], tok_send, tok_recv.at[b, f], ep=(z + step) * X + x
        )

    def onward(b, f, way):
        step = s if way == IN else -s
        to = jnp.where((step < 0) & (z + step == b), Z, b)
        return send(
            acc.at[b, f], acc.at[to, f], acc_send, acc_recv.at[to, f], ep=(z + step) * X + x
        )

    def to_line(i):
        return send(
            meta.at[z], meta.at[z], meta_send.at[i], meta_recv.at[z], ep=lax.rem(z + i, Z) * X + x
        )

    def to_plane(i, kind, j):
        q = g * WG + j
        piece = wbuf.at[x, c, kind, q]
        return send(
            piece, piece, wx_send.at[i], plane_sem.at[x, kind, j], ep=z * X + lax.rem(x + i, X)
        )

    def to_group(p, i, kind, j):
        piece = wbuf.at[p, c, kind, g * WG + j]
        return send(
            piece, piece, wy_send.at[p, i], group_sem.at[p, g, kind, j], grp=lax.rem(g + i, G)
        )

    def native_to_core(kind):
        block = wbuf.at[x, c, kind]
        return send(block, block, wt_send.at[x], nat_sem.at[kind], tp=other)

    def to_core(p, kind, q):
        piece = wbuf.at[p, c, kind, q]
        rsem = down_sem.at[p, q // SUB] if kind == 2 else wide_sem.at[p, kind]
        return send(piece, piece, wt_send.at[p], rsem, tp=other)

    for i in range(1, Z):
        to_line(i).start()
    for f in range(F):
        pl.when(is_inner)(lambda f=f: along(z, f, OUT).start())
        if f < LEAD:
            along(z, f, IN).start()
        else:
            pl.when(is_end)(lambda f=f: along(z, f, IN).start())
    for kind in range(3):
        if kind > 0:
            load_own(kind).wait()
        for j in range(WG):
            for i in range(1, X):
                to_plane(i, kind, j).start()
        native_to_core(kind).start()
    gain_copy = send(gain_out_ref, gains.at[1], gain_send, gain_recv, tp=other)
    gain_copy.start()

    PIECES = 3 * WG

    def tick(n):
        if n < PIECES:
            kind, j = n // WG, n % WG
            q = g * WG + j
            for i in range(1, X):
                p = lax.rem(x + i, X)
                arrived(wbuf.at[p, c, kind, q], plane_sem.at[p, kind, j])
                for i2 in range(1, G):
                    to_group(p, i2, kind, j).start()
                to_core(p, kind, q).start()
        if LAG <= n < PIECES + LAG:
            kind, j = (n - LAG) // WG, (n - LAG) % WG
            for i in range(1, X):
                p = lax.rem(x + i, X)
                for i2 in range(1, G):
                    g2 = lax.rem(g + i2, G)
                    q = g2 * WG + j
                    arrived(wbuf.at[p, c, kind, q], group_sem.at[p, g2, kind, j])
                    to_core(p, kind, q).start()

    def native_slices(kind):
        arrived(wbuf.at[x, other, kind], nat_sem.at[kind])

    def core_slices(kind):
        for i in range(1, X):
            p = lax.rem(x + i, X)
            arrived(wbuf.at[p, other, kind], wide_sem.at[p, kind])

    def down_slices(f):
        for i in range(1, X):
            p = lax.rem(x + i, X)
            arrived(wbuf.at[p, other, 2, pl.ds(f * SUB, SUB)], down_sem.at[p, f])

    def lines():
        for i in range(1, Z):
            b = lax.rem(z + i, Z)
            arrived(meta.at[b], meta_recv.at[b])

    def route(b):
        m = meta[b]
        expert = (lax.broadcasted_iota(jnp.int32, (8, T), 0) + z * X).astype(jnp.float32)
        first, second = m[0:1] == expert, m[1:2] == expert
        named = jnp.where(first | second, 1.0, 0.0)
        gate_row = jnp.where(first, m[2:3], 0.0) + jnp.where(second, m[3:4], 0.0)
        line = lax.broadcasted_iota(jnp.int32, (T, T), 0)
        earlier = jnp.where(line < lax.broadcasted_iota(jnp.int32, (T, T), 1), 1.0, 0.0)
        before = jnp.dot(
            named.astype(jnp.bfloat16), earlier.astype(jnp.bfloat16), preferred_element_type=jnp.float32
        )
        place = jnp.where(named > 0.0, before, -1.0)
        slot = lax.broadcasted_iota(jnp.int32, (cap, T), 0).astype(jnp.float32)
        for p in range(X):
            hit = place[p : p + 1] == slot
            pick[b, p * cap : (p + 1) * cap] = jnp.where(hit, 1.0, 0.0).astype(jnp.bfloat16)
            weight = jnp.sum(jnp.where(hit, gate_row[p : p + 1], 0.0), axis=1, keepdims=True)
            gslot[b, p * cap : (p + 1) * cap] = jnp.broadcast_to(weight, (cap, 128))

    def gather(b):
        square = jnp.zeros((R, 1), jnp.float32)
        for f in range(F):
            row = jnp.dot(pick[b], tok[b, f], preferred_element_type=jnp.float32)
            square = square + jnp.sum(row * row, axis=1, keepdims=True)
            rows[:, f * C : (f + 1) * C] = row.astype(jnp.bfloat16)
        inv = lax.rsqrt(square / D + EPS)
        for f in range(F):
            span = slice(f * C, (f + 1) * C)
            rows[:, span] = (rows[:, span].astype(jnp.float32) * inv * gain_in_ref[:, span]).astype(jnp.bfloat16)

    def gate(b):
        for p in range(X):
            for half in range(2):
                gated[p * cap : (p + 1) * cap, half * H : (half + 1) * H] = jnp.dot(
                    rows[p * cap : (p + 1) * cap], wbuf[p, half, 0].reshape(D, H),
                    preferred_element_type=jnp.float32,
                )

    def up(b, p):
        span = pl.ds(pl.multiple_of(p * cap, cap), cap)
        for half in range(2):
            side = slice(half * H, (half + 1) * H)
            wide = jnp.dot(rows[span], wbuf[p, half, 1].reshape(D, H), preferred_element_type=jnp.float32)
            value = gated[span, side]
            hid[b, span, side] = (value / (1.0 + jnp.exp(-value)) * wide).astype(jnp.bfloat16)

    def hidden(b):
        route(b)
        gather(b)
        gate(b)
        for p in range(X):
            up(b, p)

    def partial(b, f):
        parts = []
        for p in range(X):
            span = slice(p * cap, (p + 1) * cap)
            low = wbuf[p, 0, 2, pl.ds(f * SUB, SUB)].reshape(C, H)
            high = wbuf[p, 1, 2, pl.ds(f * SUB, SUB)].reshape(C, H)
            y = lax.dot_general(
                hid[b, span, 0:H], low, NT, preferred_element_type=jnp.float32
            ) + lax.dot_general(
                hid[b, span, H : 2 * H], high, NT, preferred_element_type=jnp.float32
            )
            parts.append((y * gslot[b, span, 0:1]).astype(jnp.bfloat16))
        return lax.dot_general(
            pick[b], jnp.concatenate(parts, axis=0), TN, preferred_element_type=jnp.float32
        )

    def own_part():
        def one(f, carry):
            comb[f] = partial(z, f)
            return carry

        lax.fori_loop(0, F, one, 0)

    def begin(b, f):
        acc[b, f] = partial(b, f).astype(jnp.bfloat16)
        onward(b, f, IN).start()

    def chain(b, f, way):
        part = partial(b, f)
        arrived(acc.at[b, f], acc_recv.at[b, f])
        acc[b, f] = (part + acc[b, f].astype(jnp.float32)).astype(jnp.bfloat16)
        onward(b, f, way).start()

    near, mid, far = z + s, z + 2 * s, z + 3 * s
    back = z - s

    @pl.when(is_end)
    def _():
        for n in range(2 * WG):
            tick(n)
            if n == WG // 2:
                lines()
                route(near)
        for f in range(F):
            arrived(tok.at[near, f], tok_recv.at[near, f])
        gather(near)
        tick(2 * WG)
        native_slices(0)
        core_slices(0)
        gate(near)
        tick(2 * WG + 1)
        native_slices(1)
        up(near, x)
        tick(2 * WG + 2)
        core_slices(1)
        for i in range(1, X):
            up(near, lax.rem(x + i, X))
        native_slices(2)
        for j in range(FG):
            if j < FG - 1:
                down_slices(g * FG + j)
                begin(near, g * FG + j)
            for k in range(SUB):
                tick(2 * WG + LAG + j * SUB + k)
            if j < FG - 1:
                for i in range(1, G):
                    f = lax.rem(g + i, G) * FG + j
                    down_slices(f)
                    begin(near, f)
        for i in range(G):
            down_slices(i * FG + FG - 1)
        for i in range(G - 1):
            begin(near, i * FG + FG - 1)

        def later(i, carry):
            b = jnp.where(i == 0, far, jnp.where(i == 1, z, mid))

            @pl.when(i != 1)
            def _():
                for f in range(F):
                    arrived(tok.at[b, f], tok_recv.at[b, f])

            hidden(b)

            @pl.when(i != 1)
            def _():
                def one(f, inner):
                    begin(b, f)
                    return inner

                lax.fori_loop(0, F, one, 0)

            pl.when(i == 1)(own_part)
            return carry

        lax.fori_loop(0, 3, later, 0)
        begin(near, F - 1)

    @pl.when(is_inner)
    def _():
        def relay(b, f, way):
            arrived(tok.at[b, f], tok_recv.at[b, f])
            along(b, f, way).start()

        for n in range(PIECES + LAG):
            tick(n)
            k = n // SUB
            if n % SUB == SUB - 1 and k < F:
                relay(back, k, IN)
                if k == F - 1:
                    for f in range(LEAD, F):
                        along(z, f, IN).start()
            k = (n - WG - 1) // SUB
            if n > WG and (n - WG - 1) % SUB == 0 and k < F:
                relay(mid, k, OUT)
        for f in range(F - 4):
            relay(near, f, OUT)
        lines()
        for kind in range(3):
            native_slices(kind)
            if kind < 2:
                core_slices(kind)
        for f in range(F):
            down_slices(f)

        def ready(i, carry):
            relay(near, F - 4 + i, OUT)
            hidden(jnp.where(i == 0, back, jnp.where(i == 1, mid, jnp.where(i == 2, z, near))))
            return carry

        lax.fori_loop(0, 4, ready, 0)
        own_part()

        def cross(i, carry):
            k, turn = i // 2, lax.rem(i, 2)
            pl.when((turn == 0) & (k < F))(lambda: chain(mid, k, IN))
            pl.when((turn == 1) & (k >= 2))(lambda: chain(back, k - 2, OUT))
            return carry

        lax.fori_loop(0, 2 * (F + 2), cross, 0)

        def last(f, carry):
            chain(near, f, IN)
            return carry

        lax.fori_loop(0, F, last, 0)

    total = jnp.zeros((T, 1), jnp.float32)
    for f in range(F):

        @pl.when(z > 0)
        def _():
            arrived(acc.at[z, f], acc_recv.at[z, f])
            comb[f] = comb[f] + acc[z, f].astype(jnp.float32)

        @pl.when(z < Z - 1)
        def _():
            arrived(acc.at[Z, f], acc_recv.at[Z, f])
            comb[f] = comb[f] + acc[Z, f].astype(jnp.float32)

        value = comb[f]
        total = total + jnp.sum(value * value, axis=1, keepdims=True)
    scale = lax.rsqrt(total / D + EPS)
    arrived(gains.at[1], gain_recv)
    half = F // 2

    def out_copy(f):
        return send(
            stage.at[f], out_ref.at[c, :, f * C : (f + 1) * C], out_send, out_recv, tp=other
        )

    for f in range(half):
        stage[f] = (comb[other * half + f] * scale * gains[1, :, f * C : (f + 1) * C]).astype(jnp.bfloat16)
        out_copy(f).start()
    for f in range(half):
        out_ref[c, :, f * C : (f + 1) * C] = (
            comb[c * half + f] * scale * gains[0, :, f * C : (f + 1) * C]
        ).astype(jnp.bfloat16)

    gain_copy.wait_send()
    for i in range(1, Z):
        to_line(i).wait_send()
    for i in range(1, X):
        p = lax.rem(x + i, X)
        arrived(wbuf.at[x, c, :, pl.ds(0, WG)], wx_send.at[i])
        for i2 in range(1, G):
            arrived(wbuf.at[p, c, :, pl.ds(0, WG)], wy_send.at[p, i2])
    for p in range(X):
        arrived(wbuf.at[p, c], wt_send.at[p])
    pl.when(is_end)(lambda: arrived(tok.at[z], tok_send))
    pl.when(is_inner)(lambda: arrived(acc, tok_send))
    arrived(acc.at[pl.ds(0, 3)], acc_send)
    arrived(stage, out_send)
    arrived(stage, out_recv)


def per_device(G, X, Z, tokens, gain_in, expert_ids, gate_weights, w_gate, w_up, w_down, gain_out):
    T, D = tokens.shape
    top = expert_ids.shape[1]
    cap = 2 * T * top // (X * Z)
    H = w_gate.shape[2]
    quad = Z == 4
    F = 8 if quad else 4
    C = D // F
    vmem = pl.BlockSpec(memory_space=pltpu.VMEM)
    hbm = pl.BlockSpec(memory_space=pl.ANY)
    bf16, f32 = jnp.bfloat16, jnp.float32
    dma = pltpu.SemaphoreType.DMA
    R = X * cap
    if quad:
        W = 2 * F
        body, pieces = quad_kernel, (W, D // W, H)
        routing, specs = (expert_ids.T, gate_weights.T), [hbm, hbm]
        scratch = [
            pltpu.VMEM((X, 2, 3, W, D // W, H), bf16),
            pltpu.VMEM((Z, F, T, C), bf16),
            pltpu.VMEM((Z, 8, T), f32),
            pltpu.VMEM((Z + 1, F, T, C), bf16),
            pltpu.VMEM((F, T, C), f32),
            pltpu.VMEM((R, D), bf16),
            pltpu.VMEM((R, 2 * H), f32),
            pltpu.VMEM((Z, R, 2 * H), bf16),
            pltpu.VMEM((Z, R, T), bf16),
            pltpu.VMEM((Z, R, 128), f32),
            pltpu.VMEM((2, 1, D // 2), f32),
            pltpu.VMEM((F // 2, T, C), bf16),
            pltpu.VMEM((top, T), jnp.int32),
            pltpu.VMEM((top, T), f32),
            dma((3,)),
            dma((3,)),
            dma((X, 3, W // G)),
            dma((X, G, 3, W // G)),
            dma((X, 2)),
            dma((X, F)),
            dma((X,)),
            dma((X, G)),
            dma((X,)),
            dma((Z, F)),
            dma,
            dma((Z,)),
            dma((Z,)),
            dma((Z + 1, F)),
            dma,
            dma,
            dma,
            dma,
            dma,
            dma,
            dma((2,)),
        ]
    else:
        first = lax.axis_index("tp") * T
        ids = lax.dynamic_slice_in_dim(expert_ids, first, T, 0).astype(f32)
        gates = lax.dynamic_slice_in_dim(gate_weights, first, T, 0)
        meta = jnp.concatenate([ids.T, gates.T, jnp.zeros((8 - 2 * top, T), f32)], axis=0)
        body, pieces = kernel, (F, C, H)
        routing, specs = (meta,), [vmem]
        scratch = [
            pltpu.VMEM((X, 2, 3, F, C, H), bf16),
            pltpu.VMEM((Z, F, T, C), bf16),
            pltpu.VMEM((Z, 8, T), f32),
            pltpu.VMEM((Z + 1, F, T, C), bf16),
            pltpu.VMEM((F, T, C), f32),
            pltpu.VMEM((R, D), bf16),
            pltpu.VMEM((Z, R, 2 * H), bf16),
            pltpu.VMEM((Z, R, T), bf16),
            pltpu.VMEM((Z, R, 128), f32),
            pltpu.VMEM((2, 1, D // 2), f32),
            pltpu.VMEM((F // 2, T, C), bf16),
            dma((X, 2, 3, F)),
            dma((X, 3, F // G)),
            dma((X, G, 3, F // G)),
            dma((X, 3, F)),
            dma((Z, F)),
            dma((2, Z, F)),
            dma((Z,)),
            dma((Z,)),
            dma((Z + 1, F)),
            dma((Z, F)),
            dma((2,)),
            dma((2,)),
            dma((F,)),
        ]
    out = pl.pallas_call(
        functools.partial(body, G, X, Z, F, cap),
        out_shape=jax.ShapeDtypeStruct((2, T, D // 2), bf16),
        in_specs=[hbm, vmem] + specs + [hbm, hbm, hbm, vmem],
        out_specs=vmem,
        scratch_shapes=scratch,
        compiler_params=pltpu.CompilerParams(
            collective_id=0, has_side_effects=True, vmem_limit_bytes=67043328
        ),
    )(
        tokens, gain_in.reshape(1, D), *routing,
        w_gate.reshape(pieces), w_up.reshape(pieces), w_down.reshape(pieces),
        gain_out.reshape(1, D // 2),
    )
    return out.reshape(2 * T, D // 2)


def solution(mesh):
    placed = (
        P(("grp", "ep", "tp"), None),
        P(),
        P(("grp", "ep"), None),
        P(("grp", "ep"), None),
        P("ep", None, "tp"),
        P("ep", None, "tp"),
        P("ep", None, "tp"),
        P("tp"),
    )
    X = plane_width(mesh.shape["ep"])
    body = functools.partial(per_device, mesh.shape["grp"], X, mesh.shape["ep"] // X)
    return jax.shard_map(
        body, mesh=mesh, in_specs=placed, out_specs=P(("grp", "ep"), "tp"), check_vma=False
    )
```

```python
import functools

import jax
import jax.numpy as jnp
from jax import lax
from jax.experimental import pallas as pl
from jax.experimental.pallas import tpu as pltpu
from jax.sharding import PartitionSpec as P

EPS = 1e-06
MESH = pl.DeviceIdType.MESH
NT = (((1,), (1,)), ((), ()))
TN = (((0,), (0,)), ((), ()))


def plane_width(ep):
    return max(n for n in range(1, ep + 1) if ep % n == 0 and n**3 <= ep)


def kernel(
    G, X, Z, F, cap,
    tokens_ref, gain_in_ref, meta_ref, wg_ref, wu_ref, wd_ref, gain_out_ref,
    out_ref,
    wbuf, tok, meta, acc, comb, rows, hid, pick, gslot, gains, inbox,
    wsem, wx_send, wy_send, wt_send, tok_recv, tok_send, meta_recv, meta_send,
    acc_recv, acc_send, misc_recv, misc_send, load_sem,
):
    g, ep, c = lax.axis_index("grp"), lax.axis_index("ep"), lax.axis_index("tp")
    z, x = ep // X, lax.rem(ep, X)
    other = 1 - c
    T = tokens_ref.shape[0]
    D = tokens_ref.shape[1]
    C = D // F
    H = wg_ref.shape[-1]
    FG = F // G
    weights = (wg_ref, wu_ref, wd_ref)

    def arrived(ref, sem):
        pltpu.make_async_copy(ref, ref, sem).wait()

    def send(src, dst, ssem, rsem, **where):
        return pltpu.make_async_remote_copy(
            src_ref=src, dst_ref=dst, send_sem=ssem, recv_sem=rsem,
            device_id=where, device_id_type=MESH,
        )

    def wslice(p, half, kind, q):
        return wbuf.at[p, half, kind, q]

    def load(f):
        return pltpu.make_async_copy(tokens_ref.at[:, f * C : (f + 1) * C], tok.at[z, f], load_sem.at[f])

    for f in range(F):
        load(f).start()

    for kind in range(3):
        for q in range(F):
            pltpu.make_async_copy(
                weights[kind].at[q], wslice(x, c, kind, q), wsem.at[x, c, kind, q]
            ).start()

    barrier = pltpu.get_barrier_semaphore()
    for i in range(1, Z):
        pl.semaphore_signal(barrier, inc=1, device_id={"ep": lax.rem(z + i, Z) * X + x}, device_id_type=MESH)
    for i in range(1, X):
        pl.semaphore_signal(barrier, inc=1, device_id={"ep": z * X + lax.rem(x + i, X)}, device_id_type=MESH)
    for i in range(1, G):
        pl.semaphore_signal(barrier, inc=1, device_id={"grp": lax.rem(g + i, G)}, device_id_type=MESH)
    pl.semaphore_signal(barrier, inc=1, device_id={"tp": other}, device_id_type=MESH)

    square = jnp.zeros((T, 1), jnp.float32)
    for f in range(F):
        load(f).wait()
        value = tok[z, f].astype(jnp.float32)
        square = square + jnp.sum(value * value, axis=1, keepdims=True)
    inv = lax.rsqrt(square / D + EPS)
    for f in range(F):
        gain = gain_in_ref[:, f * C : (f + 1) * C]
        tok[z, f] = (tok[z, f].astype(jnp.float32) * inv * gain).astype(jnp.bfloat16)

    pl.semaphore_wait(barrier, Z + X + G - 2)

    def to_line(i):
        return send(
            meta_ref, meta.at[z], meta_send.at[i], meta_recv.at[z], ep=lax.rem(z + i, Z) * X + x
        )

    for i in range(1, Z):
        to_line(i).start()

    def along(b, f, way):
        step = 1 if way == 0 else -1
        return send(
            tok.at[b, f], tok.at[b, f], tok_send.at[way, b, f], tok_recv.at[b, f], ep=(z + step) * X + x
        )

    can = (z < Z - 1, z > 0)
    for f in range(F):
        for way in range(2):
            pl.when(can[way])(lambda f=f, way=way: along(z, f, way).start())

    def to_plane(i, kind, j):
        q = g * FG + j
        return send(
            weights[kind].at[q], wslice(x, c, kind, q), wx_send.at[i, kind, j],
            wsem.at[x, c, kind, q], ep=z * X + lax.rem(x + i, X),
        )

    for kind in range(3):
        for j in range(FG):
            for i in range(1, X):
                to_plane(i, kind, j).start()

    gain_copy = send(gain_out_ref, gains.at[1], misc_send.at[0], misc_recv.at[0], tp=other)
    gain_copy.start()
    gains[0] = gain_out_ref[...]
    meta[z] = meta_ref[...]

    def to_core(p, kind, q):
        return send(
            wslice(p, c, kind, q), wslice(p, c, kind, q), wt_send.at[p, kind, q],
            wsem.at[p, c, kind, q], tp=other,
        )

    def to_group(p, i, kind, j):
        q = g * FG + j
        return send(
            wslice(p, c, kind, q), wslice(p, c, kind, q), wy_send.at[p, i, kind, j],
            wsem.at[p, c, kind, q], grp=lax.rem(g + i, G),
        )

    for kind in range(3):
        for q in range(F):
            arrived(wslice(x, c, kind, q), wsem.at[x, c, kind, q])
            to_core(x, kind, q).start()

    def from_plane(n):
        kind, j = n // FG, n % FG
        q = g * FG + j
        for i in range(1, X):
            p = lax.rem(x + i, X)
            arrived(wslice(p, c, kind, q), wsem.at[p, c, kind, q])
            for i2 in range(1, G):
                to_group(p, i2, kind, j).start()
            to_core(p, kind, q).start()

    def from_group(n):
        kind, j = n // FG, n % FG
        for i in range(1, X):
            p = lax.rem(x + i, X)
            for i2 in range(1, G):
                q = lax.rem(g + i2, G) * FG + j
                arrived(wslice(p, c, kind, q), wsem.at[p, c, kind, q])
                to_core(p, kind, q).start()

    def from_core(kind):
        for p in range(X):
            for q in range(F):
                arrived(wslice(p, other, kind, q), wsem.at[p, other, kind, q])

    def relay(d, f):
        for way in range(2):
            b = z - d if way == 0 else z + d
            have = b >= 0 if way == 0 else b < Z

            @pl.when(have)
            def _():
                arrived(tok.at[b, f], tok_recv.at[b, f])
                pl.when(can[way])(lambda: along(b, f, way).start())

    def hidden(b):
        m = meta[b]
        expert = (lax.broadcasted_iota(jnp.int32, (8, T), 0) + z * X).astype(jnp.float32)
        first, second = m[0:1] == expert, m[1:2] == expert
        named = jnp.where(first | second, 1.0, 0.0)
        gate = jnp.where(first, m[2:3], 0.0) + jnp.where(second, m[3:4], 0.0)
        line = lax.broadcasted_iota(jnp.int32, (T, T), 0)
        earlier = jnp.where(line < lax.broadcasted_iota(jnp.int32, (T, T), 1), 1.0, 0.0)
        before = jnp.dot(
            named.astype(jnp.bfloat16), earlier.astype(jnp.bfloat16), preferred_element_type=jnp.float32
        )
        place = jnp.where(named > 0.0, before, -1.0)
        slot = lax.broadcasted_iota(jnp.int32, (cap, T), 0).astype(jnp.float32)
        for p in range(X):
            hit = place[p : p + 1] == slot
            pick[b, p * cap : (p + 1) * cap] = jnp.where(hit, 1.0, 0.0).astype(jnp.bfloat16)
            weight = jnp.sum(jnp.where(hit, gate[p : p + 1], 0.0), axis=1, keepdims=True)
            gslot[b, p * cap : (p + 1) * cap] = jnp.broadcast_to(weight, (cap, 128))
        for f in range(F):
            rows[:, f * C : (f + 1) * C] = jnp.dot(
                pick[b], tok[b, f], preferred_element_type=jnp.float32
            ).astype(jnp.bfloat16)
        for p in range(X):
            here = rows[p * cap : (p + 1) * cap]
            for half in range(2):
                gated = jnp.dot(here, wbuf[p, half, 0].reshape(D, H), preferred_element_type=jnp.float32)
                up = jnp.dot(here, wbuf[p, half, 1].reshape(D, H), preferred_element_type=jnp.float32)
                value = gated / (1.0 + jnp.exp(-gated)) * up
                hid[b, p * cap : (p + 1) * cap, half * H : (half + 1) * H] = value.astype(jnp.bfloat16)

    def partial(b, f):
        parts = []
        for p in range(X):
            span = slice(p * cap, (p + 1) * cap)
            y = lax.dot_general(
                hid[b, span, 0:H], wbuf[p, 0, 2, f], NT, preferred_element_type=jnp.float32
            ) + lax.dot_general(
                hid[b, span, H : 2 * H], wbuf[p, 1, 2, f], NT, preferred_element_type=jnp.float32
            )
            parts.append((y * gslot[b, span, 0:1]).astype(jnp.bfloat16))
        return lax.dot_general(
            pick[b], jnp.concatenate(parts, axis=0), TN, preferred_element_type=jnp.float32
        )

    def both_hidden(d):
        def side(s, carry):
            b = z + d * (2 * s - 1)
            pl.when((b >= 0) & (b < Z))(lambda: hidden(b))
            return carry

        lax.fori_loop(0, 2, side, 0)

    def onward(b, f, way):
        step = 1 - 2 * way
        to = jnp.where((way == 1) & (z - 1 == b), Z, b)
        return send(
            acc.at[b, f], acc.at[to, f], acc_send.at[b, f], acc_recv.at[to, f], ep=(z + step) * X + x
        )

    def sums(d, low, high):
        def chunk(i, carry):
            f = i // 2
            turn = lax.rem(i, 2)
            way = jnp.where(2 * z < Z, turn, 1 - turn)
            b = jnp.where(way == 0, d, Z - 1 - d)
            active = jnp.where(way == 0, b - z, z - b) > 0
            fed = jnp.where(way == 0, z, Z - 1 - z) > 0

            @pl.when(active & fed)
            def _():
                part = partial(b, f)
                arrived(acc.at[b, f], acc_recv.at[b, f])
                acc[b, f] = (part + acc[b, f].astype(jnp.float32)).astype(jnp.bfloat16)
                onward(b, f, way).start()

            @pl.when(active & jnp.logical_not(fed))
            def _():
                acc[b, f] = partial(b, f).astype(jnp.bfloat16)
                onward(b, f, way).start()

            return carry

        lax.fori_loop(2 * low, 2 * high, chunk, 0)

    pieces = 3 * FG
    for n in range(max(pieces, F)):
        if n < F:
            relay(1, n)
        elif Z > 2 and n - F < F:
            relay(2, n - F)
        if n < pieces:
            from_plane(n)
        if 1 <= n <= pieces:
            from_group(n - 1)
    if pieces >= F:
        from_group(pieces - 1)
    done = max(pieces, F) - F
    for i in range(1, Z):
        b = lax.rem(z + i, Z)
        arrived(meta.at[b], meta_recv.at[b])
    from_core(0)
    from_core(1)
    both_hidden(1)
    from_core(2)
    early = F // 4
    sums(1, 0, early)
    if Z > 2:
        for f in range(done, F):
            relay(2, f)
        both_hidden(2)

    if Z > 2:
        sums(2, 0, F)

    def stage(d, carry):
        def one(f, inner):
            relay(d, f)
            return inner

        lax.fori_loop(0, F, one, 0)
        both_hidden(d)
        sums(d, 0, F)
        return carry

    lax.fori_loop(3, Z, stage, 0)
    sums(1, early, F)

    hidden(z)
    total = jnp.zeros((T, 1), jnp.float32)
    for f in range(F):
        comb[f] = partial(z, f)
    for f in range(F):

        @pl.when(z > 0)
        def _():
            arrived(acc.at[z, f], acc_recv.at[z, f])
            comb[f] = comb[f] + acc[z, f].astype(jnp.float32)

        @pl.when(z < Z - 1)
        def _():
            arrived(acc.at[Z, f], acc_recv.at[Z, f])
            comb[f] = comb[f] + acc[Z, f].astype(jnp.float32)

        value = comb[f]
        total = total + jnp.sum(value * value, axis=1, keepdims=True)
    scale = lax.rsqrt(total / D + EPS)
    arrived(gains.at[1], misc_recv.at[0])
    half = F // 2
    for f in range(F):
        pl.when(can[0])(lambda f=f: along(z, f, 0).wait_send())
        pl.when(can[1])(lambda f=f: along(z, f, 1).wait_send())
    for f in range(half):
        gain = gains[1, :, f * C : (f + 1) * C]
        tok[z, f] = (comb[other * half + f] * scale * gain).astype(jnp.bfloat16)
    out_copy = send(tok.at[z, :half], inbox, misc_send.at[1], misc_recv.at[1], tp=other)
    out_copy.start()
    for f in range(half):
        gain = gains[0, :, f * C : (f + 1) * C]
        out_ref[c, :, f * C : (f + 1) * C] = (comb[c * half + f] * scale * gain).astype(jnp.bfloat16)

    gain_copy.wait_send()
    for i in range(1, Z):
        to_line(i).wait_send()
    for kind in range(3):
        for i in range(1, X):
            p = lax.rem(x + i, X)
            for j in range(FG):
                to_plane(i, kind, j).wait_send()
                for i2 in range(1, G):
                    to_group(p, i2, kind, j).wait_send()
        for p in range(X):
            for q in range(F):
                to_core(p, kind, q).wait_send()

    def drain(b, carry):
        for f in range(F):
            pl.when(can[0] & (b < z))(lambda f=f: along(b, f, 0).wait_send())
            pl.when(can[1] & (b > z))(lambda f=f: along(b, f, 1).wait_send())
            pl.when(b != z)(lambda f=f: onward(b, f, 0).wait_send())
        return carry

    lax.fori_loop(0, Z, drain, 0)
    out_copy.wait()
    for f in range(half):
        out_ref[other, :, f * C : (f + 1) * C] = inbox[f]


def quad_kernel(
    G, X, Z, F, cap,
    tokens_ref, gain_in_ref, ids_ref, gates_ref, wg_ref, wu_ref, wd_ref, gain_out_ref,
    out_ref,
    wbuf, tok, meta, acc, comb, rows, gated, hid, pick, gslot, gains, stage, ids, gates, gain_row,
    own_sem, nat_sem, plane_sem, group_sem, wide_sem, down_sem, wx_send, wy_send, wt_send,
    tok_recv, tok_send, meta_recv, meta_send, acc_recv, acc_send,
    gain_recv, gain_send, out_recv, out_send, load_sem, pair_sem,
):
    g, ep, c = lax.axis_index("grp"), lax.axis_index("ep"), lax.axis_index("tp")
    z, x = ep // X, lax.rem(ep, X)
    other = 1 - c
    T, D = tokens_ref.shape
    C = D // F
    W, C2, H = wg_ref.shape
    R = X * cap
    FG, WG = F // G, W // G
    SUB = W // F
    LEAD = F // 2
    LAG = 3
    weights = (wg_ref, wu_ref, wd_ref)
    is_end = (z == 0) | (z == Z - 1)
    is_inner = jnp.logical_not(is_end)
    s = jnp.where(2 * z < Z, 1, -1)
    IN, OUT = 0, 1

    def arrived(ref, sem):
        pltpu.make_async_copy(ref, ref, sem).wait()

    def send(src, dst, ssem, rsem, **where):
        return pltpu.make_async_remote_copy(
            src_ref=src, dst_ref=dst, send_sem=ssem, recv_sem=rsem,
            device_id=where, device_id_type=MESH,
        )

    def load(f):
        return pltpu.make_async_copy(
            tokens_ref.at[:, f * C : (f + 1) * C], tok.at[z, f], load_sem.at[f // LEAD]
        )

    def load_own(kind):
        return pltpu.make_async_copy(weights[kind], wbuf.at[x, c, kind], own_sem.at[kind])

    mine = pl.ds(pl.multiple_of(c * T, T), T)
    small = (
        pltpu.make_async_copy(ids_ref.at[:, mine], ids, pair_sem.at[0]),
        pltpu.make_async_copy(gates_ref.at[:, mine], gates, pair_sem.at[1]),
        pltpu.make_async_copy(gain_out_ref, gains.at[0], pair_sem.at[2]),
        pltpu.make_async_copy(gain_in_ref, gain_row, pair_sem.at[3]),
    )
    for f in range(LEAD):
        load(f).start()
    load_own(0).start()

    barrier = pltpu.get_barrier_semaphore()
    for i in range(1, Z):
        pl.semaphore_signal(barrier, inc=1, device_id={"ep": lax.rem(z + i, Z) * X + x}, device_id_type=MESH)
    for i in range(1, X):
        pl.semaphore_signal(barrier, inc=1, device_id={"ep": z * X + lax.rem(x + i, X)}, device_id_type=MESH)
    for i in range(1, G):
        pl.semaphore_signal(barrier, inc=1, device_id={"grp": lax.rem(g + i, G)}, device_id_type=MESH)
    pl.semaphore_signal(barrier, inc=1, device_id={"tp": other}, device_id_type=MESH)
    for piece in small:
        piece.start()
    for f in range(LEAD, F):
        load(f).start()
    pl.semaphore_wait(barrier, Z + X + G - 2)

    def along(b, f, way):
        step = s if way == IN else -s
        return send(
            tok.at[b, f], tok.at[b, f], tok_send, tok_recv.at[lax.rem(b - z - step + Z, Z) - 1, f],
            ep=(z + step) * X + x,
        )

    def token(b, f):
        arrived(tok.at[b, f], tok_recv.at[lax.rem(b - z + Z, Z) - 1, f])

    def onward(b, f, way):
        step = s if way == IN else -s
        to = jnp.where((step < 0) & (z + step == b), Z, b)
        return send(
            acc.at[b, f], acc.at[to, f], acc_send, acc_recv.at[to, f], ep=(z + step) * X + x
        )

    def to_line(i):
        return send(
            meta.at[z], meta.at[z], meta_send.at[i], meta_recv.at[z], ep=lax.rem(z + i, Z) * X + x
        )

    def to_plane(i, kind, j):
        q = g * WG + j
        piece = wbuf.at[x, c, kind, q]
        return send(
            piece, piece, wx_send.at[i], plane_sem.at[X - i - 1, kind, j],
            ep=z * X + lax.rem(x + i, X),
        )

    def ahead(p):
        return lax.rem(p - x + X, X) - 1

    def to_group(p, i, kind, j):
        piece = wbuf.at[p, c, kind, g * WG + j]
        return send(
            piece, piece, wy_send.at[p, i], group_sem.at[ahead(p), G - i - 1, kind, j],
            grp=lax.rem(g + i, G),
        )

    def native_to_core(kind):
        block = wbuf.at[x, c, kind]
        return send(block, block, wt_send.at[x], nat_sem.at[kind], tp=other)

    def to_core(p, kind, q):
        piece = wbuf.at[p, c, kind, q]
        rsem = down_sem.at[ahead(p), q // SUB] if kind == 2 else wide_sem.at[ahead(p), kind]
        return send(piece, piece, wt_send.at[p], rsem, tp=other)

    def own_tokens(low, high):
        arrived(tok.at[z, pl.ds(low, high - low)], load_sem.at[low // LEAD])
        for f in range(low, high):
            pl.when(is_inner)(lambda f=f: along(z, f, OUT).start())
            if f < LEAD:
                along(z, f, IN).start()
            else:
                pl.when(is_end)(lambda f=f: along(z, f, IN).start())

    def own_weights(kind):
        load_own(kind).wait()
        for j in range(WG):
            for i in range(1, X):
                to_plane(i, kind, j).start()
        native_to_core(kind).start()

    own_tokens(0, LEAD)
    own_weights(0)
    load_own(1).start()
    load_own(2).start()
    for piece in small:
        piece.wait()
    meta[z] = jnp.concatenate(
        [ids[...].astype(jnp.float32), gates[...], jnp.zeros((8 - 2 * ids.shape[0], T), jnp.float32)], axis=0
    )
    gain_copy = send(gains.at[0], gains.at[1], gain_send, gain_recv, tp=other)
    gain_copy.start()
    for i in range(1, Z):
        to_line(i).start()
    own_tokens(LEAD, F)
    own_weights(1)
    own_weights(2)

    PIECES = 3 * WG

    def tick(n):
        if n < PIECES:
            kind, j = n // WG, n % WG
            q = g * WG + j
            for i in range(1, X):
                p = lax.rem(x + i, X)
                arrived(wbuf.at[p, c, kind, q], plane_sem.at[i - 1, kind, j])
                for i2 in range(1, G):
                    to_group(p, i2, kind, j).start()
                to_core(p, kind, q).start()
        if LAG <= n < PIECES + LAG:
            kind, j = (n - LAG) // WG, (n - LAG) % WG
            for i in range(1, X):
                p = lax.rem(x + i, X)
                for i2 in range(1, G):
                    g2 = lax.rem(g + i2, G)
                    q = g2 * WG + j
                    arrived(wbuf.at[p, c, kind, q], group_sem.at[i - 1, i2 - 1, kind, j])
                    to_core(p, kind, q).start()

    def native_slices(kind):
        arrived(wbuf.at[x, other, kind], nat_sem.at[kind])

    def core_slices(kind):
        for i in range(1, X):
            p = lax.rem(x + i, X)
            arrived(wbuf.at[p, other, kind], wide_sem.at[i - 1, kind])

    def down_slices(f):
        for i in range(1, X):
            p = lax.rem(x + i, X)
            arrived(wbuf.at[p, other, 2, pl.ds(f * SUB, SUB)], down_sem.at[i - 1, f])

    def lines():
        for i in range(1, Z):
            b = lax.rem(z + i, Z)
            arrived(meta.at[b], meta_recv.at[b])

    def route(b):
        m = meta[b]
        expert = (lax.broadcasted_iota(jnp.int32, (8, T), 0) + z * X).astype(jnp.float32)
        first, second = m[0:1] == expert, m[1:2] == expert
        named = jnp.where(first | second, 1.0, 0.0)
        gate_row = jnp.where(first, m[2:3], 0.0) + jnp.where(second, m[3:4], 0.0)
        line = lax.broadcasted_iota(jnp.int32, (T, T), 0)
        earlier = jnp.where(line < lax.broadcasted_iota(jnp.int32, (T, T), 1), 1.0, 0.0)
        before = jnp.dot(
            named.astype(jnp.bfloat16), earlier.astype(jnp.bfloat16), preferred_element_type=jnp.float32
        )
        place = jnp.where(named > 0.0, before, -1.0)
        slot = lax.broadcasted_iota(jnp.int32, (cap, T), 0).astype(jnp.float32)
        for p in range(X):
            hit = place[p : p + 1] == slot
            pick[b, p * cap : (p + 1) * cap] = jnp.where(hit, 1.0, 0.0).astype(jnp.bfloat16)
            weight = jnp.sum(jnp.where(hit, gate_row[p : p + 1], 0.0), axis=1, keepdims=True)
            gslot[b, p * cap : (p + 1) * cap] = jnp.broadcast_to(weight, (cap, 128))

    def gather(b):
        square = jnp.zeros((R, 1), jnp.float32)
        for f in range(F):
            row = jnp.dot(pick[b], tok[b, f], preferred_element_type=jnp.float32)
            square = square + jnp.sum(row * row, axis=1, keepdims=True)
            rows[:, f * C : (f + 1) * C] = row.astype(jnp.bfloat16)
        inv = lax.rsqrt(square / D + EPS)
        for f in range(F):
            span = slice(f * C, (f + 1) * C)
            rows[:, span] = (rows[:, span].astype(jnp.float32) * inv * gain_row[:, span]).astype(jnp.bfloat16)

    def gate(b):
        for p in range(X):
            for half in range(2):
                gated[p * cap : (p + 1) * cap, half * H : (half + 1) * H] = jnp.dot(
                    rows[p * cap : (p + 1) * cap], wbuf[p, half, 0].reshape(D, H),
                    preferred_element_type=jnp.float32,
                )

    def up(b, p):
        span = pl.ds(pl.multiple_of(p * cap, cap), cap)
        for half in range(2):
            side = slice(half * H, (half + 1) * H)
            wide = jnp.dot(rows[span], wbuf[p, half, 1].reshape(D, H), preferred_element_type=jnp.float32)
            value = gated[span, side]
            hid[b, span, side] = (value / (1.0 + jnp.exp(-value)) * wide).astype(jnp.bfloat16)

    def hidden(b):
        route(b)
        gather(b)
        gate(b)
        for p in range(X):
            up(b, p)

    def partial(b, f):
        parts = []
        for p in range(X):
            span = slice(p * cap, (p + 1) * cap)
            low = wbuf[p, 0, 2, pl.ds(f * SUB, SUB)].reshape(C, H)
            high = wbuf[p, 1, 2, pl.ds(f * SUB, SUB)].reshape(C, H)
            y = lax.dot_general(
                hid[b, span, 0:H], low, NT, preferred_element_type=jnp.float32
            ) + lax.dot_general(
                hid[b, span, H : 2 * H], high, NT, preferred_element_type=jnp.float32
            )
            parts.append((y * gslot[b, span, 0:1]).astype(jnp.bfloat16))
        return lax.dot_general(
            pick[b], jnp.concatenate(parts, axis=0), TN, preferred_element_type=jnp.float32
        )

    def own_part():
        def one(f, carry):
            comb[f] = partial(z, f)
            return carry

        lax.fori_loop(0, F, one, 0)

    def begin(b, f):
        acc[b, f] = partial(b, f).astype(jnp.bfloat16)
        onward(b, f, IN).start()

    def chain(b, f, way):
        part = partial(b, f)
        arrived(acc.at[b, f], acc_recv.at[b, f])
        acc[b, f] = (part + acc[b, f].astype(jnp.float32)).astype(jnp.bfloat16)
        onward(b, f, way).start()

    near, mid, far = z + s, z + 2 * s, z + 3 * s
    back = z - s

    @pl.when(is_end)
    def _():
        for n in range(2 * WG):
            tick(n)
            if n == WG // 2:
                lines()
                route(near)
        for f in range(F):
            token(near, f)
        gather(near)
        tick(2 * WG)
        native_slices(0)
        core_slices(0)
        gate(near)
        tick(2 * WG + 1)
        native_slices(1)
        up(near, x)
        tick(2 * WG + 2)
        core_slices(1)
        for i in range(1, X):
            up(near, lax.rem(x + i, X))
        native_slices(2)
        for j in range(FG):
            if j < FG - 1:
                down_slices(g * FG + j)
                begin(near, g * FG + j)
            for k in range(SUB):
                tick(2 * WG + LAG + j * SUB + k)
            if j < FG - 1:
                for i in range(1, G):
                    f = lax.rem(g + i, G) * FG + j
                    down_slices(f)
                    begin(near, f)
        for i in range(G):
            down_slices(i * FG + FG - 1)
        for i in range(G - 1):
            begin(near, i * FG + FG - 1)

        def later(i, carry):
            b = jnp.where(i == 0, far, jnp.where(i == 1, z, mid))

            @pl.when(i != 1)
            def _():
                for f in range(F):
                    token(b, f)

            hidden(b)

            @pl.when(i != 1)
            def _():
                def one(f, inner):
                    begin(b, f)
                    return inner

                lax.fori_loop(0, F, one, 0)

            pl.when(i == 1)(own_part)
            return carry

        lax.fori_loop(0, 3, later, 0)
        begin(near, F - 1)

    @pl.when(is_inner)
    def _():
        def relay(b, f, way):
            token(b, f)
            along(b, f, way).start()

        for n in range(PIECES + LAG):
            tick(n)
            k = n // SUB
            if n % SUB == SUB - 1 and k < F:
                relay(back, k, IN)
                if k == F - 1:
                    for f in range(LEAD, F):
                        along(z, f, IN).start()
            k = (n - WG - 1) // SUB
            if n > WG and (n - WG - 1) % SUB == 0 and k < F:
                relay(mid, k, OUT)
        for f in range(F - 4):
            relay(near, f, OUT)
        lines()
        for kind in range(3):
            native_slices(kind)
            if kind < 2:
                core_slices(kind)
        for f in range(F):
            down_slices(f)

        def ready(i, carry):
            relay(near, F - 4 + i, OUT)
            hidden(jnp.where(i == 0, back, jnp.where(i == 1, mid, jnp.where(i == 2, z, near))))
            return carry

        lax.fori_loop(0, 4, ready, 0)
        own_part()

        def cross(i, carry):
            k, turn = i // 2, lax.rem(i, 2)
            pl.when(turn == 0)(lambda: chain(jnp.where(k < F, mid, near), lax.rem(k, F), IN))
            pl.when((turn == 1) & (k >= 2) & (k < F + 2))(lambda: chain(back, k - 2, OUT))
            return carry

        lax.fori_loop(0, 4 * F, cross, 0)

    total = jnp.zeros((T, 1), jnp.float32)
    for f in range(F):

        @pl.when(z > 0)
        def _():
            arrived(acc.at[z, f], acc_recv.at[z, f])
            comb[f] = comb[f] + acc[z, f].astype(jnp.float32)

        @pl.when(z < Z - 1)
        def _():
            arrived(acc.at[Z, f], acc_recv.at[Z, f])
            comb[f] = comb[f] + acc[Z, f].astype(jnp.float32)

        value = comb[f]
        total = total + jnp.sum(value * value, axis=1, keepdims=True)
    scale = lax.rsqrt(total / D + EPS)
    arrived(gains.at[1], gain_recv)
    half = F // 2

    def out_copy(f):
        return send(
            stage.at[f], out_ref.at[c, :, f * C : (f + 1) * C], out_send, out_recv, tp=other
        )

    for f in range(half):
        stage[f] = (comb[other * half + f] * scale * gains[1, :, f * C : (f + 1) * C]).astype(jnp.bfloat16)
        out_copy(f).start()
    for f in range(half):
        out_ref[c, :, f * C : (f + 1) * C] = (
            comb[c * half + f] * scale * gains[0, :, f * C : (f + 1) * C]
        ).astype(jnp.bfloat16)

    gain_copy.wait_send()
    for i in range(1, Z):
        to_line(i).wait_send()
    for i in range(1, X):
        p = lax.rem(x + i, X)
        arrived(wbuf.at[x, c, :, pl.ds(0, WG)], wx_send.at[i])
        for i2 in range(1, G):
            arrived(wbuf.at[p, c, :, pl.ds(0, WG)], wy_send.at[p, i2])
    for p in range(X):
        arrived(wbuf.at[p, c], wt_send.at[p])
    pl.when(is_end)(lambda: arrived(tok.at[z], tok_send))
    pl.when(is_inner)(lambda: arrived(acc, tok_send))
    arrived(acc.at[pl.ds(0, 3)], acc_send)
    arrived(stage, out_send)
    arrived(stage, out_recv)


def per_device(G, X, Z, tokens, gain_in, expert_ids, gate_weights, w_gate, w_up, w_down, gain_out):
    T, D = tokens.shape
    top = expert_ids.shape[1]
    cap = 2 * T * top // (X * Z)
    H = w_gate.shape[2]
    quad = Z == 4
    F = 8 if quad else 4
    C = D // F
    vmem = pl.BlockSpec(memory_space=pltpu.VMEM)
    hbm = pl.BlockSpec(memory_space=pl.ANY)
    bf16, f32 = jnp.bfloat16, jnp.float32
    dma = pltpu.SemaphoreType.DMA
    R = X * cap
    if quad:
        W = 2 * F
        body, pieces = quad_kernel, (W, D // W, H)
        routing, specs = (expert_ids.T, gate_weights.T), [hbm] * 8
        scratch = [
            pltpu.VMEM((X, 2, 3, W, D // W, H), bf16),
            pltpu.VMEM((Z, F, T, C), bf16),
            pltpu.VMEM((Z, 8, T), f32),
            pltpu.VMEM((Z + 1, F, T, C), bf16),
            pltpu.VMEM((F, T, C), f32),
            pltpu.VMEM((R, D), bf16),
            pltpu.VMEM((R, 2 * H), f32),
            pltpu.VMEM((Z, R, 2 * H), bf16),
            pltpu.VMEM((Z, R, T), bf16),
            pltpu.VMEM((Z, R, 128), f32),
            pltpu.VMEM((2, 1, D // 2), f32),
            pltpu.VMEM((F // 2, T, C), bf16),
            pltpu.VMEM((top, T), jnp.int32),
            pltpu.VMEM((top, T), f32),
            pltpu.VMEM((1, D), f32),
            dma((3,)),
            dma((3,)),
            dma((X - 1, 3, W // G)),
            dma((X - 1, G - 1, 3, W // G)),
            dma((X - 1, 2)),
            dma((X - 1, F)),
            dma((X,)),
            dma((X, G)),
            dma((X,)),
            dma((Z - 1, F)),
            dma,
            dma((Z,)),
            dma((Z,)),
            dma((Z + 1, F)),
            dma,
            dma,
            dma,
            dma,
            dma,
            dma((2,)),
            dma((4,)),
        ]
        out_type = pltpu.VMEM((2, T, D // 2), bf16)
        limit = 67043328 - 2 * T * D
    else:
        first = lax.axis_index("tp") * T
        ids = lax.dynamic_slice_in_dim(expert_ids, first, T, 0).astype(f32)
        gates = lax.dynamic_slice_in_dim(gate_weights, first, T, 0)
        meta = jnp.concatenate([ids.T, gates.T, jnp.zeros((8 - 2 * top, T), f32)], axis=0)
        body, pieces = kernel, (F, C, H)
        routing, specs = (meta,), [hbm, vmem, vmem, hbm, hbm, hbm, vmem]
        out_type = jax.ShapeDtypeStruct((2, T, D // 2), bf16)
        limit = 67043328
        scratch = [
            pltpu.VMEM((X, 2, 3, F, C, H), bf16),
            pltpu.VMEM((Z, F, T, C), bf16),
            pltpu.VMEM((Z, 8, T), f32),
            pltpu.VMEM((Z + 1, F, T, C), bf16),
            pltpu.VMEM((F, T, C), f32),
            pltpu.VMEM((R, D), bf16),
            pltpu.VMEM((Z, R, 2 * H), bf16),
            pltpu.VMEM((Z, R, T), bf16),
            pltpu.VMEM((Z, R, 128), f32),
            pltpu.VMEM((2, 1, D // 2), f32),
            pltpu.VMEM((F // 2, T, C), bf16),
            dma((X, 2, 3, F)),
            dma((X, 3, F // G)),
            dma((X, G, 3, F // G)),
            dma((X, 3, F)),
            dma((Z, F)),
            dma((2, Z, F)),
            dma((Z,)),
            dma((Z,)),
            dma((Z + 1, F)),
            dma((Z, F)),
            dma((2,)),
            dma((2,)),
            dma((F,)),
        ]
    out = pl.pallas_call(
        functools.partial(body, G, X, Z, F, cap),
        out_shape=out_type,
        in_specs=specs,
        out_specs=vmem,
        scratch_shapes=scratch,
        compiler_params=pltpu.CompilerParams(
            collective_id=0, has_side_effects=True, vmem_limit_bytes=limit
        ),
    )(
        tokens, gain_in.reshape(1, D), *routing,
        w_gate.reshape(pieces), w_up.reshape(pieces), w_down.reshape(pieces),
        gain_out.reshape(1, D // 2),
    )
    return out.reshape(2 * T, D // 2)


def solution(mesh):
    placed = (
        P(("grp", "ep", "tp"), None),
        P(),
        P(("grp", "ep"), None),
        P(("grp", "ep"), None),
        P("ep", None, "tp"),
        P("ep", None, "tp"),
        P("ep", None, "tp"),
        P("tp"),
    )
    X = plane_width(mesh.shape["ep"])
    body = functools.partial(per_device, mesh.shape["grp"], X, mesh.shape["ep"] // X)
    return jax.shard_map(
        body, mesh=mesh, in_specs=placed, out_specs=P(("grp", "ep"), "tp"), check_vma=False
    )
```

```python
import functools

import jax
import jax.numpy as jnp
from jax import lax
from jax.experimental import pallas as pl
from jax.experimental.pallas import tpu as pltpu
from jax.sharding import PartitionSpec as P

EPS = 1e-06
MESH = pl.DeviceIdType.MESH
NT = (((1,), (1,)), ((), ()))
TN = (((0,), (0,)), ((), ()))


def plane_width(ep):
    return max(n for n in range(1, ep + 1) if ep % n == 0 and n**3 <= ep)


def kernel(
    G, X, Z, F, cap,
    tokens_ref, gain_in_ref, meta_ref, wg_ref, wu_ref, wd_ref, gain_out_ref,
    out_ref,
    wbuf, tok, meta, acc, comb, rows, hid, pick, gslot, gains, inbox,
    wsem, wx_send, wy_send, wt_send, tok_recv, tok_send, meta_recv, meta_send,
    acc_recv, acc_send, misc_recv, misc_send, load_sem,
):
    g, ep, c = lax.axis_index("grp"), lax.axis_index("ep"), lax.axis_index("tp")
    z, x = ep // X, lax.rem(ep, X)
    other = 1 - c
    T = tokens_ref.shape[0]
    D = tokens_ref.shape[1]
    C = D // F
    H = wg_ref.shape[-1]
    FG = F // G
    weights = (wg_ref, wu_ref, wd_ref)

    def arrived(ref, sem):
        pltpu.make_async_copy(ref, ref, sem).wait()

    def send(src, dst, ssem, rsem, **where):
        return pltpu.make_async_remote_copy(
            src_ref=src, dst_ref=dst, send_sem=ssem, recv_sem=rsem,
            device_id=where, device_id_type=MESH,
        )

    def wslice(p, half, kind, q):
        return wbuf.at[p, half, kind, q]

    def load(f):
        return pltpu.make_async_copy(tokens_ref.at[:, f * C : (f + 1) * C], tok.at[z, f], load_sem.at[f])

    for f in range(F):
        load(f).start()

    for kind in range(3):
        for q in range(F):
            pltpu.make_async_copy(
                weights[kind].at[q], wslice(x, c, kind, q), wsem.at[x, c, kind, q]
            ).start()

    barrier = pltpu.get_barrier_semaphore()
    for i in range(1, Z):
        pl.semaphore_signal(barrier, inc=1, device_id={"ep": lax.rem(z + i, Z) * X + x}, device_id_type=MESH)
    for i in range(1, X):
        pl.semaphore_signal(barrier, inc=1, device_id={"ep": z * X + lax.rem(x + i, X)}, device_id_type=MESH)
    for i in range(1, G):
        pl.semaphore_signal(barrier, inc=1, device_id={"grp": lax.rem(g + i, G)}, device_id_type=MESH)
    pl.semaphore_signal(barrier, inc=1, device_id={"tp": other}, device_id_type=MESH)

    square = jnp.zeros((T, 1), jnp.float32)
    for f in range(F):
        load(f).wait()
        value = tok[z, f].astype(jnp.float32)
        square = square + jnp.sum(value * value, axis=1, keepdims=True)
    inv = lax.rsqrt(square / D + EPS)
    for f in range(F):
        gain = gain_in_ref[:, f * C : (f + 1) * C]
        tok[z, f] = (tok[z, f].astype(jnp.float32) * inv * gain).astype(jnp.bfloat16)

    pl.semaphore_wait(barrier, Z + X + G - 2)

    def to_line(i):
        return send(
            meta_ref, meta.at[z], meta_send.at[i], meta_recv.at[z], ep=lax.rem(z + i, Z) * X + x
        )

    for i in range(1, Z):
        to_line(i).start()

    def along(b, f, way):
        step = 1 if way == 0 else -1
        return send(
            tok.at[b, f], tok.at[b, f], tok_send.at[way, b, f], tok_recv.at[b, f], ep=(z + step) * X + x
        )

    can = (z < Z - 1, z > 0)
    for f in range(F):
        for way in range(2):
            pl.when(can[way])(lambda f=f, way=way: along(z, f, way).start())

    def to_plane(i, kind, j):
        q = g * FG + j
        return send(
            weights[kind].at[q], wslice(x, c, kind, q), wx_send.at[i, kind, j],
            wsem.at[x, c, kind, q], ep=z * X + lax.rem(x + i, X),
        )

    for kind in range(3):
        for j in range(FG):
            for i in range(1, X):
                to_plane(i, kind, j).start()

    gain_copy = send(gain_out_ref, gains.at[1], misc_send.at[0], misc_recv.at[0], tp=other)
    gain_copy.start()
    gains[0] = gain_out_ref[...]
    meta[z] = meta_ref[...]

    def to_core(p, kind, q):
        return send(
            wslice(p, c, kind, q), wslice(p, c, kind, q), wt_send.at[p, kind, q],
            wsem.at[p, c, kind, q], tp=other,
        )

    def to_group(p, i, kind, j):
        q = g * FG + j
        return send(
            wslice(p, c, kind, q), wslice(p, c, kind, q), wy_send.at[p, i, kind, j],
            wsem.at[p, c, kind, q], grp=lax.rem(g + i, G),
        )

    for kind in range(3):
        for q in range(F):
            arrived(wslice(x, c, kind, q), wsem.at[x, c, kind, q])
            to_core(x, kind, q).start()

    def from_plane(n):
        kind, j = n // FG, n % FG
        q = g * FG + j
        for i in range(1, X):
            p = lax.rem(x + i, X)
            arrived(wslice(p, c, kind, q), wsem.at[p, c, kind, q])
            for i2 in range(1, G):
                to_group(p, i2, kind, j).start()
            to_core(p, kind, q).start()

    def from_group(n):
        kind, j = n // FG, n % FG
        for i in range(1, X):
            p = lax.rem(x + i, X)
            for i2 in range(1, G):
                q = lax.rem(g + i2, G) * FG + j
                arrived(wslice(p, c, kind, q), wsem.at[p, c, kind, q])
                to_core(p, kind, q).start()

    def from_core(kind):
        for p in range(X):
            for q in range(F):
                arrived(wslice(p, other, kind, q), wsem.at[p, other, kind, q])

    def relay(d, f):
        for way in range(2):
            b = z - d if way == 0 else z + d
            have = b >= 0 if way == 0 else b < Z

            @pl.when(have)
            def _():
                arrived(tok.at[b, f], tok_recv.at[b, f])
                pl.when(can[way])(lambda: along(b, f, way).start())

    def hidden(b):
        m = meta[b]
        expert = (lax.broadcasted_iota(jnp.int32, (8, T), 0) + z * X).astype(jnp.float32)
        first, second = m[0:1] == expert, m[1:2] == expert
        named = jnp.where(first | second, 1.0, 0.0)
        gate = jnp.where(first, m[2:3], 0.0) + jnp.where(second, m[3:4], 0.0)
        line = lax.broadcasted_iota(jnp.int32, (T, T), 0)
        earlier = jnp.where(line < lax.broadcasted_iota(jnp.int32, (T, T), 1), 1.0, 0.0)
        before = jnp.dot(
            named.astype(jnp.bfloat16), earlier.astype(jnp.bfloat16), preferred_element_type=jnp.float32
        )
        place = jnp.where(named > 0.0, before, -1.0)
        slot = lax.broadcasted_iota(jnp.int32, (cap, T), 0).astype(jnp.float32)
        for p in range(X):
            hit = place[p : p + 1] == slot
            pick[b, p * cap : (p + 1) * cap] = jnp.where(hit, 1.0, 0.0).astype(jnp.bfloat16)
            weight = jnp.sum(jnp.where(hit, gate[p : p + 1], 0.0), axis=1, keepdims=True)
            gslot[b, p * cap : (p + 1) * cap] = jnp.broadcast_to(weight, (cap, 128))
        for f in range(F):
            rows[:, f * C : (f + 1) * C] = jnp.dot(
                pick[b], tok[b, f], preferred_element_type=jnp.float32
            ).astype(jnp.bfloat16)
        for p in range(X):
            here = rows[p * cap : (p + 1) * cap]
            for half in range(2):
                gated = jnp.dot(here, wbuf[p, half, 0].reshape(D, H), preferred_element_type=jnp.float32)
                up = jnp.dot(here, wbuf[p, half, 1].reshape(D, H), preferred_element_type=jnp.float32)
                value = gated / (1.0 + jnp.exp(-gated)) * up
                hid[b, p * cap : (p + 1) * cap, half * H : (half + 1) * H] = value.astype(jnp.bfloat16)

    def partial(b, f):
        parts = []
        for p in range(X):
            span = slice(p * cap, (p + 1) * cap)
            y = lax.dot_general(
                hid[b, span, 0:H], wbuf[p, 0, 2, f], NT, preferred_element_type=jnp.float32
            ) + lax.dot_general(
                hid[b, span, H : 2 * H], wbuf[p, 1, 2, f], NT, preferred_element_type=jnp.float32
            )
            parts.append((y * gslot[b, span, 0:1]).astype(jnp.bfloat16))
        return lax.dot_general(
            pick[b], jnp.concatenate(parts, axis=0), TN, preferred_element_type=jnp.float32
        )

    def both_hidden(d):
        def side(s, carry):
            b = z + d * (2 * s - 1)
            pl.when((b >= 0) & (b < Z))(lambda: hidden(b))
            return carry

        lax.fori_loop(0, 2, side, 0)

    def onward(b, f, way):
        step = 1 - 2 * way
        to = jnp.where((way == 1) & (z - 1 == b), Z, b)
        return send(
            acc.at[b, f], acc.at[to, f], acc_send.at[b, f], acc_recv.at[to, f], ep=(z + step) * X + x
        )

    def sums(d, low, high):
        def chunk(i, carry):
            f = i // 2
            turn = lax.rem(i, 2)
            way = jnp.where(2 * z < Z, turn, 1 - turn)
            b = jnp.where(way == 0, d, Z - 1 - d)
            active = jnp.where(way == 0, b - z, z - b) > 0
            fed = jnp.where(way == 0, z, Z - 1 - z) > 0

            @pl.when(active & fed)
            def _():
                part = partial(b, f)
                arrived(acc.at[b, f], acc_recv.at[b, f])
                acc[b, f] = (part + acc[b, f].astype(jnp.float32)).astype(jnp.bfloat16)
                onward(b, f, way).start()

            @pl.when(active & jnp.logical_not(fed))
            def _():
                acc[b, f] = partial(b, f).astype(jnp.bfloat16)
                onward(b, f, way).start()

            return carry

        lax.fori_loop(2 * low, 2 * high, chunk, 0)

    pieces = 3 * FG
    for n in range(max(pieces, F)):
        if n < F:
            relay(1, n)
        elif Z > 2 and n - F < F:
            relay(2, n - F)
        if n < pieces:
            from_plane(n)
        if 1 <= n <= pieces:
            from_group(n - 1)
    if pieces >= F:
        from_group(pieces - 1)
    done = max(pieces, F) - F
    for i in range(1, Z):
        b = lax.rem(z + i, Z)
        arrived(meta.at[b], meta_recv.at[b])
    from_core(0)
    from_core(1)
    both_hidden(1)
    from_core(2)
    early = F // 4
    sums(1, 0, early)
    if Z > 2:
        for f in range(done, F):
            relay(2, f)
        both_hidden(2)

    if Z > 2:
        sums(2, 0, F)

    def stage(d, carry):
        def one(f, inner):
            relay(d, f)
            return inner

        lax.fori_loop(0, F, one, 0)
        both_hidden(d)
        sums(d, 0, F)
        return carry

    lax.fori_loop(3, Z, stage, 0)
    sums(1, early, F)

    hidden(z)
    total = jnp.zeros((T, 1), jnp.float32)
    for f in range(F):
        comb[f] = partial(z, f)
    for f in range(F):

        @pl.when(z > 0)
        def _():
            arrived(acc.at[z, f], acc_recv.at[z, f])
            comb[f] = comb[f] + acc[z, f].astype(jnp.float32)

        @pl.when(z < Z - 1)
        def _():
            arrived(acc.at[Z, f], acc_recv.at[Z, f])
            comb[f] = comb[f] + acc[Z, f].astype(jnp.float32)

        value = comb[f]
        total = total + jnp.sum(value * value, axis=1, keepdims=True)
    scale = lax.rsqrt(total / D + EPS)
    arrived(gains.at[1], misc_recv.at[0])
    half = F // 2
    for f in range(F):
        pl.when(can[0])(lambda f=f: along(z, f, 0).wait_send())
        pl.when(can[1])(lambda f=f: along(z, f, 1).wait_send())
    for f in range(half):
        gain = gains[1, :, f * C : (f + 1) * C]
        tok[z, f] = (comb[other * half + f] * scale * gain).astype(jnp.bfloat16)
    out_copy = send(tok.at[z, :half], inbox, misc_send.at[1], misc_recv.at[1], tp=other)
    out_copy.start()
    for f in range(half):
        gain = gains[0, :, f * C : (f + 1) * C]
        out_ref[c, :, f * C : (f + 1) * C] = (comb[c * half + f] * scale * gain).astype(jnp.bfloat16)

    gain_copy.wait_send()
    for i in range(1, Z):
        to_line(i).wait_send()
    for kind in range(3):
        for i in range(1, X):
            p = lax.rem(x + i, X)
            for j in range(FG):
                to_plane(i, kind, j).wait_send()
                for i2 in range(1, G):
                    to_group(p, i2, kind, j).wait_send()
        for p in range(X):
            for q in range(F):
                to_core(p, kind, q).wait_send()

    def drain(b, carry):
        for f in range(F):
            pl.when(can[0] & (b < z))(lambda f=f: along(b, f, 0).wait_send())
            pl.when(can[1] & (b > z))(lambda f=f: along(b, f, 1).wait_send())
            pl.when(b != z)(lambda f=f: onward(b, f, 0).wait_send())
        return carry

    lax.fori_loop(0, Z, drain, 0)
    out_copy.wait()
    for f in range(half):
        out_ref[other, :, f * C : (f + 1) * C] = inbox[f]


def quad_kernel(
    G, X, Z, F, cap,
    tokens_ref, gain_in_ref, ids_ref, gates_ref, wg_ref, wu_ref, wd_ref, gain_out_ref,
    out_ref,
    wbuf, tok, meta, acc, comb, rows, gated, hid, pick, gslot, gains, stage, ids, gates, gain_row,
    own_sem, nat_sem, plane_sem, group_sem, wide_sem, down_sem, wx_send, wy_send, wt_send,
    tok_recv, tok_send, meta_recv, meta_send, acc_recv, acc_send,
    gain_recv, gain_send, out_recv, out_send, load_sem, pair_sem,
):
    g, ep, c = lax.axis_index("grp"), lax.axis_index("ep"), lax.axis_index("tp")
    z, x = ep // X, lax.rem(ep, X)
    other = 1 - c
    T, D = tokens_ref.shape
    C = D // F
    W, C2, H = wg_ref.shape
    R = X * cap
    FG, WG = F // G, W // G
    SUB = W // F
    LEAD = F // 2
    LAG = 3
    weights = (wg_ref, wu_ref, wd_ref)
    is_end = (z == 0) | (z == Z - 1)
    is_inner = jnp.logical_not(is_end)
    s = jnp.where(2 * z < Z, 1, -1)
    IN, OUT = 0, 1

    def arrived(ref, sem):
        pltpu.make_async_copy(ref, ref, sem).wait()

    def send(src, dst, ssem, rsem, **where):
        return pltpu.make_async_remote_copy(
            src_ref=src, dst_ref=dst, send_sem=ssem, recv_sem=rsem,
            device_id=where, device_id_type=MESH,
        )

    def load(f):
        return pltpu.make_async_copy(
            tokens_ref.at[:, f * C : (f + 1) * C], tok.at[z, f], load_sem.at[f // LEAD]
        )

    def load_own(kind):
        return pltpu.make_async_copy(weights[kind], wbuf.at[x, c, kind], own_sem.at[kind])

    mine = pl.ds(pl.multiple_of(c * T, T), T)
    small = (
        pltpu.make_async_copy(ids_ref.at[:, mine], ids, pair_sem.at[0]),
        pltpu.make_async_copy(gates_ref.at[:, mine], gates, pair_sem.at[1]),
        pltpu.make_async_copy(gain_out_ref, gains.at[0], pair_sem.at[2]),
        pltpu.make_async_copy(gain_in_ref, gain_row, pair_sem.at[3]),
    )
    for f in range(LEAD):
        load(f).start()
    load_own(0).start()

    barrier = pltpu.get_barrier_semaphore()
    for i in range(1, Z):
        pl.semaphore_signal(barrier, inc=1, device_id={"ep": lax.rem(z + i, Z) * X + x}, device_id_type=MESH)
    for i in range(1, X):
        pl.semaphore_signal(barrier, inc=1, device_id={"ep": z * X + lax.rem(x + i, X)}, device_id_type=MESH)
    for i in range(1, G):
        pl.semaphore_signal(barrier, inc=1, device_id={"grp": lax.rem(g + i, G)}, device_id_type=MESH)
    pl.semaphore_signal(barrier, inc=1, device_id={"tp": other}, device_id_type=MESH)
    for piece in small:
        piece.start()
    for f in range(LEAD, F):
        load(f).start()
    pl.semaphore_wait(barrier, Z + X + G - 2)

    def along(b, f, way):
        step = s if way == IN else -s
        return send(
            tok.at[b, f], tok.at[b, f], tok_send, tok_recv.at[lax.rem(b - z - step + Z, Z) - 1, f],
            ep=(z + step) * X + x,
        )

    def token(b, f):
        arrived(tok.at[b, f], tok_recv.at[lax.rem(b - z + Z, Z) - 1, f])

    def onward(b, f, way):
        step = s if way == IN else -s
        to = jnp.where((step < 0) & (z + step == b), Z, b)
        return send(
            acc.at[b, f], acc.at[to, f], acc_send, acc_recv.at[to, f], ep=(z + step) * X + x
        )

    def halves(b, f, h):
        return acc.at[b, f, pl.ds(h * T // 2, T // 2)]

    def onward_half(b, h, way):
        step = s if way == IN else -s
        to = jnp.where((step < 0) & (z + step == b), Z, b)
        return send(
            halves(b, F - 1, h), halves(to, F - 1, h), acc_send, acc_recv.at[to, F - 1 + h],
            ep=(z + step) * X + x,
        )

    def to_line(i):
        return send(
            meta.at[z], meta.at[z], meta_send.at[i], meta_recv.at[z], ep=lax.rem(z + i, Z) * X + x
        )

    def to_plane(i, kind, j):
        q = g * WG + j
        piece = wbuf.at[x, c, kind, q]
        return send(
            piece, piece, wx_send.at[i], plane_sem.at[X - i - 1, kind, j],
            ep=z * X + lax.rem(x + i, X),
        )

    def ahead(p):
        return lax.rem(p - x + X, X) - 1

    def to_group(p, i, kind, j):
        piece = wbuf.at[p, c, kind, g * WG + j]
        return send(
            piece, piece, wy_send.at[p, i], group_sem.at[ahead(p), G - i - 1, kind, j],
            grp=lax.rem(g + i, G),
        )

    def native_to_core(kind):
        block = wbuf.at[x, c, kind]
        return send(block, block, wt_send.at[x], nat_sem.at[kind], tp=other)

    def to_core(p, kind, q):
        piece = wbuf.at[p, c, kind, q]
        rsem = down_sem.at[ahead(p), q // SUB] if kind == 2 else wide_sem.at[ahead(p), kind]
        return send(piece, piece, wt_send.at[p], rsem, tp=other)

    def own_tokens(low, high):
        arrived(tok.at[z, pl.ds(low, high - low)], load_sem.at[low // LEAD])
        for f in range(low, high):
            pl.when(is_inner)(lambda f=f: along(z, f, OUT).start())
            if f < LEAD:
                along(z, f, IN).start()
            else:
                pl.when(is_end)(lambda f=f: along(z, f, IN).start())

    def own_weights(kind):
        for j in range(WG):
            for i in range(1, X):
                to_plane(i, kind, j).start()

    own_tokens(0, LEAD)
    load_own(0).wait()
    own_weights(0)
    native_to_core(0).start()
    load_own(1).start()
    load_own(2).start()
    for piece in small:
        piece.wait()
    meta[z] = jnp.concatenate(
        [ids[...].astype(jnp.float32), gates[...], jnp.zeros((8 - 2 * ids.shape[0], T), jnp.float32)], axis=0
    )
    gain_copy = send(gains.at[0], gains.at[1], gain_send, gain_recv, tp=other)
    gain_copy.start()
    for i in range(1, Z):
        to_line(i).start()
    own_tokens(LEAD, F)
    load_own(1).wait()
    own_weights(1)
    native_to_core(1).start()
    load_own(2).wait()
    pl.when(c == 0)(lambda: own_weights(2))
    native_to_core(2).start()

    PIECES = 3 * WG

    def tick(n):
        if n < PIECES:
            kind, j = n // WG, n % WG
            q = g * WG + j
            for i in range(1, X):
                p = lax.rem(x + i, X)
                arrived(wbuf.at[p, c, kind, q], plane_sem.at[i - 1, kind, j])
                for i2 in range(1, G):
                    to_group(p, i2, kind, j).start()
                to_core(p, kind, q).start()
        if LAG <= n < PIECES + LAG:
            kind, j = (n - LAG) // WG, (n - LAG) % WG
            for i in range(1, X):
                p = lax.rem(x + i, X)
                for i2 in range(1, G):
                    g2 = lax.rem(g + i2, G)
                    q = g2 * WG + j
                    arrived(wbuf.at[p, c, kind, q], group_sem.at[i - 1, i2 - 1, kind, j])
                    to_core(p, kind, q).start()

    def native_slices(kind):
        arrived(wbuf.at[x, other, kind], nat_sem.at[kind])

    def core_slices(kind):
        for i in range(1, X):
            p = lax.rem(x + i, X)
            arrived(wbuf.at[p, other, kind], wide_sem.at[i - 1, kind])

    def down_slices(f):
        for i in range(1, X):
            p = lax.rem(x + i, X)
            arrived(wbuf.at[p, other, 2, pl.ds(f * SUB, SUB)], down_sem.at[i - 1, f])

    def lines():
        for i in range(1, Z):
            b = lax.rem(z + i, Z)
            arrived(meta.at[b], meta_recv.at[b])

    def route(b):
        m = meta[b]
        expert = (lax.broadcasted_iota(jnp.int32, (8, T), 0) + z * X).astype(jnp.float32)
        first, second = m[0:1] == expert, m[1:2] == expert
        named = jnp.where(first | second, 1.0, 0.0)
        gate_row = jnp.where(first, m[2:3], 0.0) + jnp.where(second, m[3:4], 0.0)
        line = lax.broadcasted_iota(jnp.int32, (T, T), 0)
        earlier = jnp.where(line < lax.broadcasted_iota(jnp.int32, (T, T), 1), 1.0, 0.0)
        before = jnp.dot(
            named.astype(jnp.bfloat16), earlier.astype(jnp.bfloat16), preferred_element_type=jnp.float32
        )
        place = jnp.where(named > 0.0, before, -1.0)
        slot = lax.broadcasted_iota(jnp.int32, (cap, T), 0).astype(jnp.float32)
        for p in range(X):
            hit = place[p : p + 1] == slot
            pick[b, p * cap : (p + 1) * cap] = jnp.where(hit, 1.0, 0.0).astype(jnp.bfloat16)
            weight = jnp.sum(jnp.where(hit, gate_row[p : p + 1], 0.0), axis=1, keepdims=True)
            gslot[b, p * cap : (p + 1) * cap] = jnp.broadcast_to(weight, (cap, 128))

    def gather(b):
        square = jnp.zeros((R, 1), jnp.float32)
        for f in range(F):
            row = jnp.dot(pick[b], tok[b, f], preferred_element_type=jnp.float32)
            square = square + jnp.sum(row * row, axis=1, keepdims=True)
            rows[:, f * C : (f + 1) * C] = row.astype(jnp.bfloat16)
        inv = lax.rsqrt(square / D + EPS)
        for f in range(F):
            span = slice(f * C, (f + 1) * C)
            rows[:, span] = (rows[:, span].astype(jnp.float32) * inv * gain_row[:, span]).astype(jnp.bfloat16)

    def gate(b):
        for p in range(X):
            for half in range(2):
                gated[p * cap : (p + 1) * cap, half * H : (half + 1) * H] = jnp.dot(
                    rows[p * cap : (p + 1) * cap], wbuf[p, half, 0].reshape(D, H),
                    preferred_element_type=jnp.float32,
                )

    def up(b, p):
        span = pl.ds(pl.multiple_of(p * cap, cap), cap)
        for half in range(2):
            side = slice(half * H, (half + 1) * H)
            wide = jnp.dot(rows[span], wbuf[p, half, 1].reshape(D, H), preferred_element_type=jnp.float32)
            value = gated[span, side]
            hid[b, span, side] = (value / (1.0 + jnp.exp(-value)) * wide).astype(jnp.bfloat16)

    def hidden(b):
        route(b)
        gather(b)
        gate(b)
        for p in range(X):
            up(b, p)

    def partial(b, f):
        parts = []
        for p in range(X):
            span = slice(p * cap, (p + 1) * cap)
            low = wbuf[p, 0, 2, pl.ds(f * SUB, SUB)].reshape(C, H)
            high = wbuf[p, 1, 2, pl.ds(f * SUB, SUB)].reshape(C, H)
            y = lax.dot_general(
                hid[b, span, 0:H], low, NT, preferred_element_type=jnp.float32
            ) + lax.dot_general(
                hid[b, span, H : 2 * H], high, NT, preferred_element_type=jnp.float32
            )
            parts.append((y * gslot[b, span, 0:1]).astype(jnp.bfloat16))
        return lax.dot_general(
            pick[b], jnp.concatenate(parts, axis=0), TN, preferred_element_type=jnp.float32
        )

    def own_part():
        def one(f, carry):
            comb[f] = partial(z, f)
            return carry

        lax.fori_loop(0, F, one, 0)

    def begin(b, f):
        acc[b, f] = partial(b, f).astype(jnp.bfloat16)
        pl.when(f != F - 1)(lambda: onward(b, f, IN).start())

        @pl.when(f == F - 1)
        def _():
            for h in range(2):
                onward_half(b, h, IN).start()

    def chain(b, f, way):
        part = partial(b, f)

        @pl.when(f != F - 1)
        def _():
            arrived(acc.at[b, f], acc_recv.at[b, f])
            acc[b, f] = (part + acc[b, f].astype(jnp.float32)).astype(jnp.bfloat16)
            onward(b, f, way).start()

        @pl.when(f == F - 1)
        def _():
            for h in range(2):
                span = slice(h * T // 2, (h + 1) * T // 2)
                arrived(halves(b, F - 1, h), acc_recv.at[b, F - 1 + h])
                acc[b, F - 1, span] = (part[span] + acc[b, F - 1, span].astype(jnp.float32)).astype(jnp.bfloat16)
                onward_half(b, h, way).start()

    near, mid, far = z + s, z + 2 * s, z + 3 * s
    back = z - s

    @pl.when(is_end)
    def _():
        for n in range(2 * WG):
            tick(n)
            if n == WG // 2:
                lines()
                route(near)
        pl.when(c != 0)(lambda: own_weights(2))
        for f in range(F):
            token(near, f)
        gather(near)
        tick(2 * WG)
        native_slices(0)
        core_slices(0)
        gate(near)
        tick(2 * WG + 1)
        native_slices(1)
        up(near, x)
        tick(2 * WG + 2)
        core_slices(1)
        for i in range(1, X):
            up(near, lax.rem(x + i, X))
        native_slices(2)
        for j in range(FG):
            if j < FG - 1:
                down_slices(g * FG + j)
                begin(near, g * FG + j)
            for k in range(SUB):
                tick(2 * WG + LAG + j * SUB + k)
            if j < FG - 1:
                for i in range(1, G):
                    f = lax.rem(g + i, G) * FG + j
                    down_slices(f)
                    begin(near, f)
        for i in range(G):
            down_slices(i * FG + FG - 1)

        def later(i, carry):
            b = jnp.where(i == 0, far, jnp.where(i == 1, z, mid))

            @pl.when(i != 1)
            def _():
                for f in range(F):
                    token(b, f)

            hidden(b)

            @pl.when(i != 1)
            def _():
                def one(f, inner):
                    begin(b, f)
                    return inner

                lax.fori_loop(0, F, one, 0)

            pl.when(i == 1)(own_part)
            return carry

        lax.fori_loop(0, 3, later, 0)
        for i in range(G):
            begin(near, i * FG + FG - 1)

    @pl.when(is_inner)
    def _():
        def relay(b, f, way):
            token(b, f)
            along(b, f, way).start()

        for n in range(PIECES + LAG):
            tick(n)
            if n == 2 * WG - 1:
                pl.when(c != 0)(lambda: own_weights(2))
            k = n // SUB
            if n % SUB == SUB - 1 and k < F:
                relay(back, k, IN)
                if k == F - 1:
                    for f in range(LEAD, F):
                        along(z, f, IN).start()
            k = (n - WG - 1) // SUB
            if n > WG and (n - WG - 1) % SUB == 0 and k < F:
                relay(mid, k, OUT)
        for f in range(F - 4):
            relay(near, f, OUT)
        lines()
        for kind in range(3):
            native_slices(kind)
            if kind < 2:
                core_slices(kind)
        for f in range(F):
            down_slices(f)

        def ready(i, carry):
            relay(near, F - 4 + i, OUT)
            hidden(jnp.where(i == 0, back, jnp.where(i == 1, mid, jnp.where(i == 2, z, near))))
            return carry

        lax.fori_loop(0, 4, ready, 0)
        own_part()

        def cross(i, carry):
            k, turn = i // 2, lax.rem(i, 2)
            pl.when(turn == 0)(lambda: chain(jnp.where(k < F, mid, near), lax.rem(k, F), IN))
            pl.when((turn == 1) & (k >= 2) & (k < F + 2))(lambda: chain(back, k - 2, OUT))
            return carry

        lax.fori_loop(0, 4 * F, cross, 0)

    total = jnp.zeros((T, 1), jnp.float32)
    for f in sorted(range(F), key=lambda f: f % FG == FG - 1):

        def join(slot):
            if f < F - 1:
                arrived(acc.at[slot, f], acc_recv.at[slot, f])
            else:
                for h in range(2):
                    arrived(halves(slot, f, h), acc_recv.at[slot, f + h])
            comb[f] = comb[f] + acc[slot, f].astype(jnp.float32)

        pl.when(z > 0)(lambda: join(z))
        pl.when(z < Z - 1)(lambda: join(Z))
        value = comb[f]
        total = total + jnp.sum(value * value, axis=1, keepdims=True)
    scale = lax.rsqrt(total / D + EPS)
    arrived(gains.at[1], gain_recv)
    half = F // 2

    def out_copy(f):
        return send(
            stage.at[f], out_ref.at[c, :, f * C : (f + 1) * C], out_send, out_recv, tp=other
        )

    for f in range(half):
        stage[f] = (comb[other * half + f] * scale * gains[1, :, f * C : (f + 1) * C]).astype(jnp.bfloat16)
        out_copy(f).start()
    for f in range(half):
        out_ref[c, :, f * C : (f + 1) * C] = (
            comb[c * half + f] * scale * gains[0, :, f * C : (f + 1) * C]
        ).astype(jnp.bfloat16)

    gain_copy.wait_send()
    for i in range(1, Z):
        to_line(i).wait_send()
    for i in range(1, X):
        p = lax.rem(x + i, X)
        arrived(wbuf.at[x, c, :, pl.ds(0, WG)], wx_send.at[i])
        for i2 in range(1, G):
            arrived(wbuf.at[p, c, :, pl.ds(0, WG)], wy_send.at[p, i2])
    for p in range(X):
        arrived(wbuf.at[p, c], wt_send.at[p])
    pl.when(is_end)(lambda: arrived(tok.at[z], tok_send))
    pl.when(is_inner)(lambda: arrived(acc, tok_send))
    arrived(acc.at[pl.ds(0, 3)], acc_send)
    arrived(stage, out_send)
    arrived(stage, out_recv)


def per_device(G, X, Z, tokens, gain_in, expert_ids, gate_weights, w_gate, w_up, w_down, gain_out):
    T, D = tokens.shape
    top = expert_ids.shape[1]
    cap = 2 * T * top // (X * Z)
    H = w_gate.shape[2]
    quad = Z == 4
    F = 8 if quad else 4
    C = D // F
    vmem = pl.BlockSpec(memory_space=pltpu.VMEM)
    hbm = pl.BlockSpec(memory_space=pl.ANY)
    bf16, f32 = jnp.bfloat16, jnp.float32
    dma = pltpu.SemaphoreType.DMA
    R = X * cap
    if quad:
        W = 2 * F
        body, pieces = quad_kernel, (W, D // W, H)
        routing, specs = (expert_ids.T, gate_weights.T), [hbm] * 8
        scratch = [
            pltpu.VMEM((X, 2, 3, W, D // W, H), bf16),
            pltpu.VMEM((Z, F, T, C), bf16),
            pltpu.VMEM((Z, 8, T), f32),
            pltpu.VMEM((Z + 1, F, T, C), bf16),
            pltpu.VMEM((F, T, C), f32),
            pltpu.VMEM((R, D), bf16),
            pltpu.VMEM((R, 2 * H), f32),
            pltpu.VMEM((Z, R, 2 * H), bf16),
            pltpu.VMEM((Z, R, T), bf16),
            pltpu.VMEM((Z, R, 128), f32),
            pltpu.VMEM((2, 1, D // 2), f32),
            pltpu.VMEM((F // 2, T, C), bf16),
            pltpu.VMEM((top, T), jnp.int32),
            pltpu.VMEM((top, T), f32),
            pltpu.VMEM((1, D), f32),
            dma((3,)),
            dma((3,)),
            dma((X - 1, 3, W // G)),
            dma((X - 1, G - 1, 3, W // G)),
            dma((X - 1, 2)),
            dma((X - 1, F)),
            dma((X,)),
            dma((X, G)),
            dma((X,)),
            dma((Z - 1, F)),
            dma,
            dma((Z,)),
            dma((Z,)),
            dma((Z + 1, F + 1)),
            dma,
            dma,
            dma,
            dma,
            dma,
            dma((2,)),
            dma((4,)),
        ]
        out_type = pltpu.VMEM((2, T, D // 2), bf16)
        limit = 67043328 - 2 * T * D
    else:
        first = lax.axis_index("tp") * T
        ids = lax.dynamic_slice_in_dim(expert_ids, first, T, 0).astype(f32)
        gates = lax.dynamic_slice_in_dim(gate_weights, first, T, 0)
        meta = jnp.concatenate([ids.T, gates.T, jnp.zeros((8 - 2 * top, T), f32)], axis=0)
        body, pieces = kernel, (F, C, H)
        routing, specs = (meta,), [hbm, vmem, vmem, hbm, hbm, hbm, vmem]
        out_type = jax.ShapeDtypeStruct((2, T, D // 2), bf16)
        limit = 67043328
        scratch = [
            pltpu.VMEM((X, 2, 3, F, C, H), bf16),
            pltpu.VMEM((Z, F, T, C), bf16),
            pltpu.VMEM((Z, 8, T), f32),
            pltpu.VMEM((Z + 1, F, T, C), bf16),
            pltpu.VMEM((F, T, C), f32),
            pltpu.VMEM((R, D), bf16),
            pltpu.VMEM((Z, R, 2 * H), bf16),
            pltpu.VMEM((Z, R, T), bf16),
            pltpu.VMEM((Z, R, 128), f32),
            pltpu.VMEM((2, 1, D // 2), f32),
            pltpu.VMEM((F // 2, T, C), bf16),
            dma((X, 2, 3, F)),
            dma((X, 3, F // G)),
            dma((X, G, 3, F // G)),
            dma((X, 3, F)),
            dma((Z, F)),
            dma((2, Z, F)),
            dma((Z,)),
            dma((Z,)),
            dma((Z + 1, F)),
            dma((Z, F)),
            dma((2,)),
            dma((2,)),
            dma((F,)),
        ]
    out = pl.pallas_call(
        functools.partial(body, G, X, Z, F, cap),
        out_shape=out_type,
        in_specs=specs,
        out_specs=vmem,
        scratch_shapes=scratch,
        compiler_params=pltpu.CompilerParams(
            collective_id=0, has_side_effects=True, vmem_limit_bytes=limit
        ),
    )(
        tokens, gain_in.reshape(1, D), *routing,
        w_gate.reshape(pieces), w_up.reshape(pieces), w_down.reshape(pieces),
        gain_out.reshape(1, D // 2),
    )
    return out.reshape(2 * T, D // 2)


def solution(mesh):
    placed = (
        P(("grp", "ep", "tp"), None),
        P(),
        P(("grp", "ep"), None),
        P(("grp", "ep"), None),
        P("ep", None, "tp"),
        P("ep", None, "tp"),
        P("ep", None, "tp"),
        P("tp"),
    )
    X = plane_width(mesh.shape["ep"])
    body = functools.partial(per_device, mesh.shape["grp"], X, mesh.shape["ep"] // X)
    return jax.shard_map(
        body, mesh=mesh, in_specs=placed, out_specs=P(("grp", "ep"), "tp"), check_vma=False
    )
```

```python
import functools

import jax
import jax.numpy as jnp
from jax import lax
from jax.experimental import pallas as pl
from jax.experimental.pallas import tpu as pltpu
from jax.sharding import PartitionSpec as P

EPS = 1e-06
MESH = pl.DeviceIdType.MESH
NT = (((1,), (1,)), ((), ()))
TN = (((0,), (0,)), ((), ()))


def plane_width(ep):
    return max(n for n in range(1, ep + 1) if ep % n == 0 and n**3 <= ep)


def kernel(
    G, X, Z, F, cap,
    tokens_ref, gain_in_ref, meta_ref, wg_ref, wu_ref, wd_ref, gain_out_ref,
    out_ref,
    wbuf, tok, meta, acc, comb, rows, hid, pick, gslot, gains, inbox,
    wsem, wx_send, wy_send, wt_send, tok_recv, tok_send, meta_recv, meta_send,
    acc_recv, acc_send, misc_recv, misc_send, load_sem,
):
    g, ep, c = lax.axis_index("grp"), lax.axis_index("ep"), lax.axis_index("tp")
    z, x = ep // X, lax.rem(ep, X)
    other = 1 - c
    T = tokens_ref.shape[0]
    D = tokens_ref.shape[1]
    C = D // F
    H = wg_ref.shape[-1]
    FG = F // G
    weights = (wg_ref, wu_ref, wd_ref)

    def arrived(ref, sem):
        pltpu.make_async_copy(ref, ref, sem).wait()

    def send(src, dst, ssem, rsem, **where):
        return pltpu.make_async_remote_copy(
            src_ref=src, dst_ref=dst, send_sem=ssem, recv_sem=rsem,
            device_id=where, device_id_type=MESH,
        )

    def wslice(p, half, kind, q):
        return wbuf.at[p, half, kind, q]

    def load(f):
        return pltpu.make_async_copy(tokens_ref.at[:, f * C : (f + 1) * C], tok.at[z, f], load_sem.at[f])

    for f in range(F):
        load(f).start()

    for kind in range(3):
        for q in range(F):
            pltpu.make_async_copy(
                weights[kind].at[q], wslice(x, c, kind, q), wsem.at[x, c, kind, q]
            ).start()

    barrier = pltpu.get_barrier_semaphore()
    for i in range(1, Z):
        pl.semaphore_signal(barrier, inc=1, device_id={"ep": lax.rem(z + i, Z) * X + x}, device_id_type=MESH)
    for i in range(1, X):
        pl.semaphore_signal(barrier, inc=1, device_id={"ep": z * X + lax.rem(x + i, X)}, device_id_type=MESH)
    for i in range(1, G):
        pl.semaphore_signal(barrier, inc=1, device_id={"grp": lax.rem(g + i, G)}, device_id_type=MESH)
    pl.semaphore_signal(barrier, inc=1, device_id={"tp": other}, device_id_type=MESH)

    square = jnp.zeros((T, 1), jnp.float32)
    for f in range(F):
        load(f).wait()
        value = tok[z, f].astype(jnp.float32)
        square = square + jnp.sum(value * value, axis=1, keepdims=True)
    inv = lax.rsqrt(square / D + EPS)
    for f in range(F):
        gain = gain_in_ref[:, f * C : (f + 1) * C]
        tok[z, f] = (tok[z, f].astype(jnp.float32) * inv * gain).astype(jnp.bfloat16)

    pl.semaphore_wait(barrier, Z + X + G - 2)

    def to_line(i):
        return send(
            meta_ref, meta.at[z], meta_send.at[i], meta_recv.at[z], ep=lax.rem(z + i, Z) * X + x
        )

    for i in range(1, Z):
        to_line(i).start()

    def along(b, f, way):
        step = 1 if way == 0 else -1
        return send(
            tok.at[b, f], tok.at[b, f], tok_send.at[way, b, f], tok_recv.at[b, f], ep=(z + step) * X + x
        )

    can = (z < Z - 1, z > 0)
    for f in range(F):
        for way in range(2):
            pl.when(can[way])(lambda f=f, way=way: along(z, f, way).start())

    def to_plane(i, kind, j):
        q = g * FG + j
        return send(
            weights[kind].at[q], wslice(x, c, kind, q), wx_send.at[i, kind, j],
            wsem.at[x, c, kind, q], ep=z * X + lax.rem(x + i, X),
        )

    for kind in range(3):
        for j in range(FG):
            for i in range(1, X):
                to_plane(i, kind, j).start()

    gain_copy = send(gain_out_ref, gains.at[1], misc_send.at[0], misc_recv.at[0], tp=other)
    gain_copy.start()
    gains[0] = gain_out_ref[...]
    meta[z] = meta_ref[...]

    def to_core(p, kind, q):
        return send(
            wslice(p, c, kind, q), wslice(p, c, kind, q), wt_send.at[p, kind, q],
            wsem.at[p, c, kind, q], tp=other,
        )

    def to_group(p, i, kind, j):
        q = g * FG + j
        return send(
            wslice(p, c, kind, q), wslice(p, c, kind, q), wy_send.at[p, i, kind, j],
            wsem.at[p, c, kind, q], grp=lax.rem(g + i, G),
        )

    for kind in range(3):
        for q in range(F):
            arrived(wslice(x, c, kind, q), wsem.at[x, c, kind, q])
            to_core(x, kind, q).start()

    def from_plane(n):
        kind, j = n // FG, n % FG
        q = g * FG + j
        for i in range(1, X):
            p = lax.rem(x + i, X)
            arrived(wslice(p, c, kind, q), wsem.at[p, c, kind, q])
            for i2 in range(1, G):
                to_group(p, i2, kind, j).start()
            to_core(p, kind, q).start()

    def from_group(n):
        kind, j = n // FG, n % FG
        for i in range(1, X):
            p = lax.rem(x + i, X)
            for i2 in range(1, G):
                q = lax.rem(g + i2, G) * FG + j
                arrived(wslice(p, c, kind, q), wsem.at[p, c, kind, q])
                to_core(p, kind, q).start()

    def from_core(kind):
        for p in range(X):
            for q in range(F):
                arrived(wslice(p, other, kind, q), wsem.at[p, other, kind, q])

    def relay(d, f):
        for way in range(2):
            b = z - d if way == 0 else z + d
            have = b >= 0 if way == 0 else b < Z

            @pl.when(have)
            def _():
                arrived(tok.at[b, f], tok_recv.at[b, f])
                pl.when(can[way])(lambda: along(b, f, way).start())

    def hidden(b):
        m = meta[b]
        expert = (lax.broadcasted_iota(jnp.int32, (8, T), 0) + z * X).astype(jnp.float32)
        first, second = m[0:1] == expert, m[1:2] == expert
        named = jnp.where(first | second, 1.0, 0.0)
        gate = jnp.where(first, m[2:3], 0.0) + jnp.where(second, m[3:4], 0.0)
        line = lax.broadcasted_iota(jnp.int32, (T, T), 0)
        earlier = jnp.where(line < lax.broadcasted_iota(jnp.int32, (T, T), 1), 1.0, 0.0)
        before = jnp.dot(
            named.astype(jnp.bfloat16), earlier.astype(jnp.bfloat16), preferred_element_type=jnp.float32
        )
        place = jnp.where(named > 0.0, before, -1.0)
        slot = lax.broadcasted_iota(jnp.int32, (cap, T), 0).astype(jnp.float32)
        for p in range(X):
            hit = place[p : p + 1] == slot
            pick[b, p * cap : (p + 1) * cap] = jnp.where(hit, 1.0, 0.0).astype(jnp.bfloat16)
            weight = jnp.sum(jnp.where(hit, gate[p : p + 1], 0.0), axis=1, keepdims=True)
            gslot[b, p * cap : (p + 1) * cap] = jnp.broadcast_to(weight, (cap, 128))
        for f in range(F):
            rows[:, f * C : (f + 1) * C] = jnp.dot(
                pick[b], tok[b, f], preferred_element_type=jnp.float32
            ).astype(jnp.bfloat16)
        for p in range(X):
            here = rows[p * cap : (p + 1) * cap]
            for half in range(2):
                gated = jnp.dot(here, wbuf[p, half, 0].reshape(D, H), preferred_element_type=jnp.float32)
                up = jnp.dot(here, wbuf[p, half, 1].reshape(D, H), preferred_element_type=jnp.float32)
                value = gated / (1.0 + jnp.exp(-gated)) * up
                hid[b, p * cap : (p + 1) * cap, half * H : (half + 1) * H] = value.astype(jnp.bfloat16)

    def partial(b, f):
        parts = []
        for p in range(X):
            span = slice(p * cap, (p + 1) * cap)
            y = lax.dot_general(
                hid[b, span, 0:H], wbuf[p, 0, 2, f], NT, preferred_element_type=jnp.float32
            ) + lax.dot_general(
                hid[b, span, H : 2 * H], wbuf[p, 1, 2, f], NT, preferred_element_type=jnp.float32
            )
            parts.append((y * gslot[b, span, 0:1]).astype(jnp.bfloat16))
        return lax.dot_general(
            pick[b], jnp.concatenate(parts, axis=0), TN, preferred_element_type=jnp.float32
        )

    def both_hidden(d):
        def side(s, carry):
            b = z + d * (2 * s - 1)
            pl.when((b >= 0) & (b < Z))(lambda: hidden(b))
            return carry

        lax.fori_loop(0, 2, side, 0)

    def onward(b, f, way):
        step = 1 - 2 * way
        to = jnp.where((way == 1) & (z - 1 == b), Z, b)
        return send(
            acc.at[b, f], acc.at[to, f], acc_send.at[b, f], acc_recv.at[to, f], ep=(z + step) * X + x
        )

    def sums(d, low, high):
        def chunk(i, carry):
            f = i // 2
            turn = lax.rem(i, 2)
            way = jnp.where(2 * z < Z, turn, 1 - turn)
            b = jnp.where(way == 0, d, Z - 1 - d)
            active = jnp.where(way == 0, b - z, z - b) > 0
            fed = jnp.where(way == 0, z, Z - 1 - z) > 0

            @pl.when(active & fed)
            def _():
                part = partial(b, f)
                arrived(acc.at[b, f], acc_recv.at[b, f])
                acc[b, f] = (part + acc[b, f].astype(jnp.float32)).astype(jnp.bfloat16)
                onward(b, f, way).start()

            @pl.when(active & jnp.logical_not(fed))
            def _():
                acc[b, f] = partial(b, f).astype(jnp.bfloat16)
                onward(b, f, way).start()

            return carry

        lax.fori_loop(2 * low, 2 * high, chunk, 0)

    pieces = 3 * FG
    for n in range(max(pieces, F)):
        if n < F:
            relay(1, n)
        elif Z > 2 and n - F < F:
            relay(2, n - F)
        if n < pieces:
            from_plane(n)
        if 1 <= n <= pieces:
            from_group(n - 1)
    if pieces >= F:
        from_group(pieces - 1)
    done = max(pieces, F) - F
    for i in range(1, Z):
        b = lax.rem(z + i, Z)
        arrived(meta.at[b], meta_recv.at[b])
    from_core(0)
    from_core(1)
    both_hidden(1)
    from_core(2)
    early = F // 4
    sums(1, 0, early)
    if Z > 2:
        for f in range(done, F):
            relay(2, f)
        both_hidden(2)

    if Z > 2:
        sums(2, 0, F)

    def stage(d, carry):
        def one(f, inner):
            relay(d, f)
            return inner

        lax.fori_loop(0, F, one, 0)
        both_hidden(d)
        sums(d, 0, F)
        return carry

    lax.fori_loop(3, Z, stage, 0)
    sums(1, early, F)

    hidden(z)
    total = jnp.zeros((T, 1), jnp.float32)
    for f in range(F):
        comb[f] = partial(z, f)
    for f in range(F):

        @pl.when(z > 0)
        def _():
            arrived(acc.at[z, f], acc_recv.at[z, f])
            comb[f] = comb[f] + acc[z, f].astype(jnp.float32)

        @pl.when(z < Z - 1)
        def _():
            arrived(acc.at[Z, f], acc_recv.at[Z, f])
            comb[f] = comb[f] + acc[Z, f].astype(jnp.float32)

        value = comb[f]
        total = total + jnp.sum(value * value, axis=1, keepdims=True)
    scale = lax.rsqrt(total / D + EPS)
    arrived(gains.at[1], misc_recv.at[0])
    half = F // 2
    for f in range(F):
        pl.when(can[0])(lambda f=f: along(z, f, 0).wait_send())
        pl.when(can[1])(lambda f=f: along(z, f, 1).wait_send())
    for f in range(half):
        gain = gains[1, :, f * C : (f + 1) * C]
        tok[z, f] = (comb[other * half + f] * scale * gain).astype(jnp.bfloat16)
    out_copy = send(tok.at[z, :half], inbox, misc_send.at[1], misc_recv.at[1], tp=other)
    out_copy.start()
    for f in range(half):
        gain = gains[0, :, f * C : (f + 1) * C]
        out_ref[c, :, f * C : (f + 1) * C] = (comb[c * half + f] * scale * gain).astype(jnp.bfloat16)

    gain_copy.wait_send()
    for i in range(1, Z):
        to_line(i).wait_send()
    for kind in range(3):
        for i in range(1, X):
            p = lax.rem(x + i, X)
            for j in range(FG):
                to_plane(i, kind, j).wait_send()
                for i2 in range(1, G):
                    to_group(p, i2, kind, j).wait_send()
        for p in range(X):
            for q in range(F):
                to_core(p, kind, q).wait_send()

    def drain(b, carry):
        for f in range(F):
            pl.when(can[0] & (b < z))(lambda f=f: along(b, f, 0).wait_send())
            pl.when(can[1] & (b > z))(lambda f=f: along(b, f, 1).wait_send())
            pl.when(b != z)(lambda f=f: onward(b, f, 0).wait_send())
        return carry

    lax.fori_loop(0, Z, drain, 0)
    out_copy.wait()
    for f in range(half):
        out_ref[other, :, f * C : (f + 1) * C] = inbox[f]


def quad_kernel(
    G, X, Z, F, cap,
    tokens_ref, gain_in_ref, ids_ref, gates_ref, wg_ref, wu_ref, wd_ref, gain_out_ref,
    out_ref,
    wbuf, tok, meta, acc, comb, rows, gated, hid, pick, gslot, gains, stage, ids, gates, gain_row,
    own_sem, nat_sem, plane_sem, group_sem, wide_sem, down_sem, wx_send, wy_send, wt_send,
    tok_recv, tok_send, meta_recv, meta_send, acc_recv, acc_send,
    gain_recv, gain_send, out_recv, out_send, load_sem, pair_sem,
):
    g, ep, c = lax.axis_index("grp"), lax.axis_index("ep"), lax.axis_index("tp")
    z, x = ep // X, lax.rem(ep, X)
    other = 1 - c
    T, D = tokens_ref.shape
    C = D // F
    W, C2, H = wg_ref.shape
    R = X * cap
    FG, WG = F // G, W // G
    SUB = W // F
    LEAD = F // 2
    LAG = 3
    weights = (wg_ref, wu_ref, wd_ref)
    is_end = (z == 0) | (z == Z - 1)
    is_inner = jnp.logical_not(is_end)
    s = jnp.where(2 * z < Z, 1, -1)
    IN, OUT = 0, 1

    def arrived(ref, sem):
        pltpu.make_async_copy(ref, ref, sem).wait()

    def send(src, dst, ssem, rsem, **where):
        return pltpu.make_async_remote_copy(
            src_ref=src, dst_ref=dst, send_sem=ssem, recv_sem=rsem,
            device_id=where, device_id_type=MESH,
        )

    def load(f):
        return pltpu.make_async_copy(
            tokens_ref.at[:, f * C : (f + 1) * C], tok.at[z, f], load_sem.at[f // LEAD]
        )

    def load_own(kind):
        return pltpu.make_async_copy(weights[kind], wbuf.at[x, c, kind], own_sem.at[kind])

    mine = pl.ds(pl.multiple_of(c * T, T), T)
    small = (
        pltpu.make_async_copy(ids_ref.at[:, mine], ids, pair_sem.at[0]),
        pltpu.make_async_copy(gates_ref.at[:, mine], gates, pair_sem.at[1]),
        pltpu.make_async_copy(gain_out_ref, gains.at[0], pair_sem.at[2]),
        pltpu.make_async_copy(gain_in_ref, gain_row, pair_sem.at[3]),
    )
    for f in range(LEAD):
        load(f).start()
    load_own(0).start()

    barrier = pltpu.get_barrier_semaphore()
    for i in range(1, Z):
        pl.semaphore_signal(barrier, inc=1, device_id={"ep": lax.rem(z + i, Z) * X + x}, device_id_type=MESH)
    for i in range(1, X):
        pl.semaphore_signal(barrier, inc=1, device_id={"ep": z * X + lax.rem(x + i, X)}, device_id_type=MESH)
    for i in range(1, G):
        pl.semaphore_signal(barrier, inc=1, device_id={"grp": lax.rem(g + i, G)}, device_id_type=MESH)
    pl.semaphore_signal(barrier, inc=1, device_id={"tp": other}, device_id_type=MESH)
    for piece in small:
        piece.start()
    for f in range(LEAD, F):
        load(f).start()
    pl.semaphore_wait(barrier, Z + X + G - 2)

    def along(b, f, way):
        step = s if way == IN else -s
        return send(
            tok.at[b, f], tok.at[b, f], tok_send, tok_recv.at[lax.rem(b - z - step + Z, Z) - 1, f],
            ep=(z + step) * X + x,
        )

    def token(b, f):
        arrived(tok.at[b, f], tok_recv.at[lax.rem(b - z + Z, Z) - 1, f])

    def onward(b, f, way):
        step = s if way == IN else -s
        to = jnp.where((step < 0) & (z + step == b), Z, b)
        return send(
            acc.at[b, f], acc.at[to, f], acc_send, acc_recv.at[to, f], ep=(z + step) * X + x
        )

    def halves(b, f, h):
        return acc.at[b, f, pl.ds(h * T // 2, T // 2)]

    def onward_half(b, h, way):
        step = s if way == IN else -s
        to = jnp.where((step < 0) & (z + step == b), Z, b)
        return send(
            halves(b, F - 1, h), halves(to, F - 1, h), acc_send, acc_recv.at[to, F - 1 + h],
            ep=(z + step) * X + x,
        )

    def to_line(i):
        return send(
            meta.at[z], meta.at[z], meta_send.at[i], meta_recv.at[z], ep=lax.rem(z + i, Z) * X + x
        )

    def to_plane(i, kind, j):
        q = g * WG + j
        piece = wbuf.at[x, c, kind, q]
        return send(
            piece, piece, wx_send.at[i], plane_sem.at[X - i - 1, kind, j],
            ep=z * X + lax.rem(x + i, X),
        )

    def ahead(p):
        return lax.rem(p - x + X, X) - 1

    def to_group(p, i, kind, j):
        piece = wbuf.at[p, c, kind, g * WG + j]
        return send(
            piece, piece, wy_send.at[p, i], group_sem.at[ahead(p), G - i - 1, kind, j],
            grp=lax.rem(g + i, G),
        )

    def native_to_core(kind):
        block = wbuf.at[x, c, kind]
        return send(block, block, wt_send.at[x], nat_sem.at[kind], tp=other)

    def to_core(p, kind, q):
        piece = wbuf.at[p, c, kind, q]
        rsem = down_sem.at[ahead(p), q // SUB] if kind == 2 else wide_sem.at[ahead(p), kind]
        return send(piece, piece, wt_send.at[p], rsem, tp=other)

    def own_tokens(low, high):
        arrived(tok.at[z, pl.ds(low, high - low)], load_sem.at[low // LEAD])
        for f in range(low, high):
            pl.when(is_inner)(lambda f=f: along(z, f, OUT).start())
            if f < LEAD:
                along(z, f, IN).start()
            else:
                pl.when(is_end)(lambda f=f: along(z, f, IN).start())

    def own_weights(kind):
        for j in range(WG):
            for i in range(1, X):
                to_plane(i, kind, j).start()

    own_tokens(0, LEAD)
    load_own(0).wait()
    own_weights(0)
    native_to_core(0).start()
    load_own(1).start()
    load_own(2).start()
    for piece in small:
        piece.wait()
    meta[z] = jnp.concatenate(
        [ids[...].astype(jnp.float32), gates[...], jnp.zeros((8 - 2 * ids.shape[0], T), jnp.float32)], axis=0
    )
    gain_copy = send(gains.at[0], gains.at[1], gain_send, gain_recv, tp=other)
    gain_copy.start()
    for i in range(1, Z):
        to_line(i).start()
    own_tokens(LEAD, F)
    load_own(1).wait()
    own_weights(1)
    native_to_core(1).start()
    load_own(2).wait()
    pl.when(c == 0)(lambda: own_weights(2))
    native_to_core(2).start()

    PIECES = 3 * WG

    def tick(n):
        if n < PIECES:
            kind, j = n // WG, n % WG
            q = g * WG + j
            for i in range(1, X):
                p = lax.rem(x + i, X)
                arrived(wbuf.at[p, c, kind, q], plane_sem.at[i - 1, kind, j])
                for i2 in range(1, G):
                    to_group(p, i2, kind, j).start()
                to_core(p, kind, q).start()
        if LAG <= n < PIECES + LAG:
            kind, j = (n - LAG) // WG, (n - LAG) % WG
            for i in range(1, X):
                p = lax.rem(x + i, X)
                for i2 in range(1, G):
                    g2 = lax.rem(g + i2, G)
                    q = g2 * WG + j
                    arrived(wbuf.at[p, c, kind, q], group_sem.at[i - 1, i2 - 1, kind, j])
                    to_core(p, kind, q).start()

    def native_slices(kind):
        arrived(wbuf.at[x, other, kind], nat_sem.at[kind])

    def core_slices(kind):
        for i in range(1, X):
            p = lax.rem(x + i, X)
            arrived(wbuf.at[p, other, kind], wide_sem.at[i - 1, kind])

    def down_slices(f):
        for i in range(1, X):
            p = lax.rem(x + i, X)
            arrived(wbuf.at[p, other, 2, pl.ds(f * SUB, SUB)], down_sem.at[i - 1, f])

    def lines():
        for i in range(1, Z):
            b = lax.rem(z + i, Z)
            arrived(meta.at[b], meta_recv.at[b])

    def route(b):
        m = meta[b]
        expert = (lax.broadcasted_iota(jnp.int32, (8, T), 0) + z * X).astype(jnp.float32)
        first, second = m[0:1] == expert, m[1:2] == expert
        named = jnp.where(first | second, 1.0, 0.0)
        gate_row = jnp.where(first, m[2:3], 0.0) + jnp.where(second, m[3:4], 0.0)
        line = lax.broadcasted_iota(jnp.int32, (T, T), 0)
        earlier = jnp.where(line < lax.broadcasted_iota(jnp.int32, (T, T), 1), 1.0, 0.0)
        before = jnp.dot(
            named.astype(jnp.bfloat16), earlier.astype(jnp.bfloat16), preferred_element_type=jnp.float32
        )
        place = jnp.where(named > 0.0, before, -1.0)
        slot = lax.broadcasted_iota(jnp.int32, (cap, T), 0).astype(jnp.float32)
        for p in range(X):
            hit = place[p : p + 1] == slot
            pick[b, p * cap : (p + 1) * cap] = jnp.where(hit, 1.0, 0.0).astype(jnp.bfloat16)
            weight = jnp.sum(jnp.where(hit, gate_row[p : p + 1], 0.0), axis=1, keepdims=True)
            gslot[b, p * cap : (p + 1) * cap] = jnp.broadcast_to(weight, (cap, 128))

    def gather(b):
        square = jnp.zeros((R, 1), jnp.float32)
        for f in range(F):
            row = jnp.dot(pick[b], tok[b, f], preferred_element_type=jnp.float32)
            square = square + jnp.sum(row * row, axis=1, keepdims=True)
            rows[:, f * C : (f + 1) * C] = row.astype(jnp.bfloat16)
        inv = lax.rsqrt(square / D + EPS)
        for f in range(F):
            span = slice(f * C, (f + 1) * C)
            rows[:, span] = (rows[:, span].astype(jnp.float32) * inv * gain_row[:, span]).astype(jnp.bfloat16)

    def gate(b):
        for p in range(X):
            for half in range(2):
                gated[p * cap : (p + 1) * cap, half * H : (half + 1) * H] = jnp.dot(
                    rows[p * cap : (p + 1) * cap], wbuf[p, half, 0].reshape(D, H),
                    preferred_element_type=jnp.float32,
                )

    def up(b, p):
        span = pl.ds(pl.multiple_of(p * cap, cap), cap)
        for half in range(2):
            side = slice(half * H, (half + 1) * H)
            wide = jnp.dot(rows[span], wbuf[p, half, 1].reshape(D, H), preferred_element_type=jnp.float32)
            value = gated[span, side]
            hid[b, span, side] = (value / (1.0 + jnp.exp(-value)) * wide).astype(jnp.bfloat16)

    def hidden(b):
        route(b)
        gather(b)
        gate(b)
        for p in range(X):
            up(b, p)

    def partial(b, f):
        parts = []
        for p in range(X):
            span = slice(p * cap, (p + 1) * cap)
            low = wbuf[p, 0, 2, pl.ds(f * SUB, SUB)].reshape(C, H)
            high = wbuf[p, 1, 2, pl.ds(f * SUB, SUB)].reshape(C, H)
            y = lax.dot_general(
                hid[b, span, 0:H], low, NT, preferred_element_type=jnp.float32
            ) + lax.dot_general(
                hid[b, span, H : 2 * H], high, NT, preferred_element_type=jnp.float32
            )
            parts.append((y * gslot[b, span, 0:1]).astype(jnp.bfloat16))
        return lax.dot_general(
            pick[b], jnp.concatenate(parts, axis=0), TN, preferred_element_type=jnp.float32
        )

    def own_part():
        def one(f, carry):
            comb[f] = partial(z, f)
            return carry

        lax.fori_loop(0, F, one, 0)

    def begin(b, f):
        acc[b, f] = partial(b, f).astype(jnp.bfloat16)
        pl.when(f != F - 1)(lambda: onward(b, f, IN).start())

        @pl.when(f == F - 1)
        def _():
            for h in range(2):
                onward_half(b, h, IN).start()

    def chain(b, f, way):
        part = partial(b, f)

        @pl.when(f != F - 1)
        def _():
            arrived(acc.at[b, f], acc_recv.at[b, f])
            acc[b, f] = (part + acc[b, f].astype(jnp.float32)).astype(jnp.bfloat16)
            onward(b, f, way).start()

        @pl.when(f == F - 1)
        def _():
            for h in range(2):
                span = slice(h * T // 2, (h + 1) * T // 2)
                arrived(halves(b, F - 1, h), acc_recv.at[b, F - 1 + h])
                acc[b, F - 1, span] = (part[span] + acc[b, F - 1, span].astype(jnp.float32)).astype(jnp.bfloat16)
                onward_half(b, h, way).start()

    near, mid, far = z + s, z + 2 * s, z + 3 * s
    back = z - s

    @pl.when(is_end)
    def _():
        for n in range(2 * WG):
            tick(n)
            if n == WG // 2:
                lines()
                route(near)
        pl.when(c != 0)(lambda: own_weights(2))
        for f in range(F):
            token(near, f)
        gather(near)
        tick(2 * WG)
        native_slices(0)
        core_slices(0)
        gate(near)
        tick(2 * WG + 1)
        native_slices(1)
        up(near, x)
        tick(2 * WG + 2)
        core_slices(1)
        for i in range(1, X):
            up(near, lax.rem(x + i, X))
        native_slices(2)
        def early(j, i):
            f = lax.rem(g + i, G) * FG + j
            down_slices(f)
            if j < FG - 1:
                begin(near, f)

        early(0, 0)
        for n in range(2 * WG + LAG, PIECES + LAG):
            tick(n)
            for j in range(FG):
                full = 2 * WG + SUB * (j + 1) - 1
                if n == full and j > 0:
                    early(j, 0)
                if n == full + LAG:
                    for i in range(1, G):
                        early(j, i)

        def later(i, carry):
            b = jnp.where(i == 0, far, jnp.where(i == 1, z, mid))

            @pl.when(i != 1)
            def _():
                for f in range(F):
                    token(b, f)

            hidden(b)

            @pl.when(i != 1)
            def _():
                def one(f, inner):
                    begin(b, f)
                    return inner

                lax.fori_loop(0, F, one, 0)

            pl.when(i == 1)(own_part)
            return carry

        lax.fori_loop(0, 3, later, 0)
        for i in range(G):
            begin(near, i * FG + FG - 1)

    @pl.when(is_inner)
    def _():
        def relay(b, f, way):
            token(b, f)
            along(b, f, way).start()

        for n in range(PIECES + LAG):
            tick(n)
            if n == 2 * WG - 1:
                pl.when(c != 0)(lambda: own_weights(2))
            k = n // SUB
            if n % SUB == SUB - 1 and k < F:
                relay(back, k, IN)
                if k == F - 1:
                    for f in range(LEAD, F):
                        along(z, f, IN).start()
            k = (n - WG - 1) // SUB
            if n > WG and (n - WG - 1) % SUB == 0 and k < F:
                relay(mid, k, OUT)
        for f in range(F - 4):
            relay(near, f, OUT)
        lines()
        for kind in range(3):
            native_slices(kind)
            if kind < 2:
                core_slices(kind)
        for f in range(F):
            down_slices(f)

        def ready(i, carry):
            relay(near, F - 4 + i, OUT)
            hidden(jnp.where(i == 0, back, jnp.where(i == 1, mid, jnp.where(i == 2, z, near))))
            return carry

        lax.fori_loop(0, 4, ready, 0)
        own_part()

        def cross(i, carry):
            k, turn = i // 2, lax.rem(i, 2)
            pl.when(turn == 0)(lambda: chain(jnp.where(k < F, mid, near), lax.rem(k, F), IN))
            pl.when((turn == 1) & (k >= 2) & (k < F + 2))(lambda: chain(back, k - 2, OUT))
            return carry

        lax.fori_loop(0, 4 * F, cross, 0)

    total = jnp.zeros((T, 1), jnp.float32)
    for f in sorted(range(F), key=lambda f: f % FG == FG - 1):

        def join(slot):
            if f < F - 1:
                arrived(acc.at[slot, f], acc_recv.at[slot, f])
            else:
                for h in range(2):
                    arrived(halves(slot, f, h), acc_recv.at[slot, f + h])
            comb[f] = comb[f] + acc[slot, f].astype(jnp.float32)

        pl.when(z > 0)(lambda: join(z))
        pl.when(z < Z - 1)(lambda: join(Z))
        value = comb[f]
        total = total + jnp.sum(value * value, axis=1, keepdims=True)
    scale = lax.rsqrt(total / D + EPS)
    arrived(gains.at[1], gain_recv)
    half = F // 2

    def out_copy(f):
        return send(
            stage.at[f], out_ref.at[c, :, f * C : (f + 1) * C], out_send, out_recv, tp=other
        )

    for f in range(half):
        stage[f] = (comb[other * half + f] * scale * gains[1, :, f * C : (f + 1) * C]).astype(jnp.bfloat16)
        out_copy(f).start()
    for f in range(half):
        out_ref[c, :, f * C : (f + 1) * C] = (
            comb[c * half + f] * scale * gains[0, :, f * C : (f + 1) * C]
        ).astype(jnp.bfloat16)

    gain_copy.wait_send()
    for i in range(1, Z):
        to_line(i).wait_send()
    for i in range(1, X):
        p = lax.rem(x + i, X)
        arrived(wbuf.at[x, c, :, pl.ds(0, WG)], wx_send.at[i])
        for i2 in range(1, G):
            arrived(wbuf.at[p, c, :, pl.ds(0, WG)], wy_send.at[p, i2])
    for p in range(X):
        arrived(wbuf.at[p, c], wt_send.at[p])
    pl.when(is_end)(lambda: arrived(tok.at[z], tok_send))
    pl.when(is_inner)(lambda: arrived(acc, tok_send))
    arrived(acc.at[pl.ds(0, 3)], acc_send)
    arrived(stage, out_send)
    arrived(stage, out_recv)


def per_device(G, X, Z, tokens, gain_in, expert_ids, gate_weights, w_gate, w_up, w_down, gain_out):
    T, D = tokens.shape
    top = expert_ids.shape[1]
    cap = 2 * T * top // (X * Z)
    H = w_gate.shape[2]
    quad = Z == 4
    F = 8 if quad else 4
    C = D // F
    vmem = pl.BlockSpec(memory_space=pltpu.VMEM)
    hbm = pl.BlockSpec(memory_space=pl.ANY)
    bf16, f32 = jnp.bfloat16, jnp.float32
    dma = pltpu.SemaphoreType.DMA
    R = X * cap
    if quad:
        W = 2 * F
        body, pieces = quad_kernel, (W, D // W, H)
        routing, specs = (expert_ids.T, gate_weights.T), [hbm] * 8
        scratch = [
            pltpu.VMEM((X, 2, 3, W, D // W, H), bf16),
            pltpu.VMEM((Z, F, T, C), bf16),
            pltpu.VMEM((Z, 8, T), f32),
            pltpu.VMEM((Z + 1, F, T, C), bf16),
            pltpu.VMEM((F, T, C), f32),
            pltpu.VMEM((R, D), bf16),
            pltpu.VMEM((R, 2 * H), f32),
            pltpu.VMEM((Z, R, 2 * H), bf16),
            pltpu.VMEM((Z, R, T), bf16),
            pltpu.VMEM((Z, R, 128), f32),
            pltpu.VMEM((2, 1, D // 2), f32),
            pltpu.VMEM((F // 2, T, C), bf16),
            pltpu.VMEM((top, T), jnp.int32),
            pltpu.VMEM((top, T), f32),
            pltpu.VMEM((1, D), f32),
            dma((3,)),
            dma((3,)),
            dma((X - 1, 3, W // G)),
            dma((X - 1, G - 1, 3, W // G)),
            dma((X - 1, 2)),
            dma((X - 1, F)),
            dma((X,)),
            dma((X, G)),
            dma((X,)),
            dma((Z - 1, F)),
            dma,
            dma((Z,)),
            dma((Z,)),
            dma((Z + 1, F + 1)),
            dma,
            dma,
            dma,
            dma,
            dma,
            dma((2,)),
            dma((4,)),
        ]
        out_type = pltpu.VMEM((2, T, D // 2), bf16)
        limit = 67043328 - 2 * T * D
    else:
        first = lax.axis_index("tp") * T
        ids = lax.dynamic_slice_in_dim(expert_ids, first, T, 0).astype(f32)
        gates = lax.dynamic_slice_in_dim(gate_weights, first, T, 0)
        meta = jnp.concatenate([ids.T, gates.T, jnp.zeros((8 - 2 * top, T), f32)], axis=0)
        body, pieces = kernel, (F, C, H)
        routing, specs = (meta,), [hbm, vmem, vmem, hbm, hbm, hbm, vmem]
        out_type = jax.ShapeDtypeStruct((2, T, D // 2), bf16)
        limit = 67043328
        scratch = [
            pltpu.VMEM((X, 2, 3, F, C, H), bf16),
            pltpu.VMEM((Z, F, T, C), bf16),
            pltpu.VMEM((Z, 8, T), f32),
            pltpu.VMEM((Z + 1, F, T, C), bf16),
            pltpu.VMEM((F, T, C), f32),
            pltpu.VMEM((R, D), bf16),
            pltpu.VMEM((Z, R, 2 * H), bf16),
            pltpu.VMEM((Z, R, T), bf16),
            pltpu.VMEM((Z, R, 128), f32),
            pltpu.VMEM((2, 1, D // 2), f32),
            pltpu.VMEM((F // 2, T, C), bf16),
            dma((X, 2, 3, F)),
            dma((X, 3, F // G)),
            dma((X, G, 3, F // G)),
            dma((X, 3, F)),
            dma((Z, F)),
            dma((2, Z, F)),
            dma((Z,)),
            dma((Z,)),
            dma((Z + 1, F)),
            dma((Z, F)),
            dma((2,)),
            dma((2,)),
            dma((F,)),
        ]
    out = pl.pallas_call(
        functools.partial(body, G, X, Z, F, cap),
        out_shape=out_type,
        in_specs=specs,
        out_specs=vmem,
        scratch_shapes=scratch,
        compiler_params=pltpu.CompilerParams(
            collective_id=0, has_side_effects=True, vmem_limit_bytes=limit
        ),
    )(
        tokens, gain_in.reshape(1, D), *routing,
        w_gate.reshape(pieces), w_up.reshape(pieces), w_down.reshape(pieces),
        gain_out.reshape(1, D // 2),
    )
    return out.reshape(2 * T, D // 2)


def solution(mesh):
    placed = (
        P(("grp", "ep", "tp"), None),
        P(),
        P(("grp", "ep"), None),
        P(("grp", "ep"), None),
        P("ep", None, "tp"),
        P("ep", None, "tp"),
        P("ep", None, "tp"),
        P("tp"),
    )
    X = plane_width(mesh.shape["ep"])
    body = functools.partial(per_device, mesh.shape["grp"], X, mesh.shape["ep"] // X)
    return jax.shard_map(
        body, mesh=mesh, in_specs=placed, out_specs=P(("grp", "ep"), "tp"), check_vma=False
    )
```
